128 devices in a mesh: rep: 16 (over z, x), fs: 4 (over y), tp: 2 (over core).
Axes of the slice: x: 4, y: 4, z: 4, core: 2. Of those that a mesh axis runs over, the one named last changes fastest.
Arguments:
- inputs: bfloat16 [64, 768, 2048], P(('rep', 'fs'), 'tp'), may hold values from -6 to 6
- pre_gate: bfloat16 [64, 768, 2816], P(('rep', 'fs'), None, 'tp'), may hold values from -6 to 6
- pre_up: bfloat16 [64, 768, 2816], P(('rep', 'fs'), None, 'tp'), may hold values from -6 to 6
- cotangent: bfloat16 [64, 768, 2816], P(('rep', 'fs'), None, 'tp'), may hold values from -16 to 16
- w_gate: bfloat16 [2048, 2816], P('fs', 'tp'), may hold values from -0.125 to 0.125
- w_up: bfloat16 [2048, 2816], P('fs', 'tp'), may hold values from -0.125 to 0.125
- taps_gate: bfloat16 [3, 2816], replicated, may hold values from -3 to 3
- taps_up: bfloat16 [3, 2816], replicated, may hold values from -3 to 3
Outputs:
- grad_inputs: bfloat16 [64, 768, 2048], P(('rep', 'fs'), 'tp')
- grad_w_gate: float32 [2048, 2816], P('fs', 'tp')
- grad_w_up: float32 [2048, 2816], P('fs', 'tp')
- grad_taps_gate: float32 [3, 2816], replicated
- grad_taps_up: float32 [3, 2816], replicated
The draws below stay inside these ranges and needn't reach their ends.
All inputs are finite; a program needn't handle non-finite values.
Results may differ from the reference program's by a relative error of at most 0.0059.
Values may be sent and summed in bfloat16 or wider, within the bound.
A program may use at most 192 MiB of HBM per device.

```python
import jax
import jax.numpy as jnp
from jax import lax

D = 2048
F = 2816
TAPS = 3
LEN = 768
SEQS = 64
TOKENS = 49152
N_TP = 2


def raised(entries, own_key, source, target, parts, factor):
    def block_of(axis_at):
        return (jnp.arange(entries.shape[axis_at]) // (entries.shape[axis_at] // parts)).reshape((-1,) + (1,) * (entries.ndim - 1 - axis_at))

    first = jax.random.permutation(own_key, parts)[block_of(target)]
    other_side = (block_of(target) + parts // 2) % parts
    return jnp.where((block_of(source) == first) | (block_of(source) == other_side), factor * entries, entries)


def levels(own_key, shape, cuts, low, top_value):
    def one(axis_at, shards_of):
        heights = jax.random.uniform(jax.random.fold_in(jax.random.fold_in(own_key, 6), axis_at), (shards_of,), jnp.float32, low / len(cuts), top_value / len(cuts))
        return jnp.repeat(jnp.exp(heights), shape[axis_at] // shards_of).reshape((-1,) + (1,) * (len(shape) - axis_at - 1))

    gain = one(*cuts[0])
    for cut in cuts[1:]:
        gain = gain * one(*cut)
    return gain


def gaussian(own_key, dims, spread, most, split=(), kind=jnp.bfloat16):
    result = spread * jax.random.normal(own_key, dims, jnp.float32)
    if split:
        result = result * levels(own_key, dims, split, -0.22, 0.18)
    return jnp.clip(result, -most, most).astype(kind)


def noise_with(own_key, shape, spread, limit, split, heavy, held_as=jnp.bfloat16):
    entries = spread * jax.random.normal(own_key, shape, jnp.float32)
    if split:
        entries = entries * levels(own_key, shape, split, -0.22, 0.18)
    return jnp.clip(raised(entries, jax.random.fold_in(own_key, 3), *heavy), -limit, limit).astype(held_as)


def setup_inputs(seed: int = 0) -> dict:
    streams_of = jax.random.split(jax.random.key(seed), 9)
    inputs = gaussian(streams_of[0], (SEQS, LEN, D), 1.0, 6.0, ((0, 64), (1, 2)))
    pre_gate = gaussian(streams_of[1], (SEQS, LEN, F), 1.0, 6.0, ((0, 64), (2, 2)))
    pre_up = gaussian(streams_of[2], (SEQS, LEN, F), 1.0, 6.0, ((0, 64), (2, 2)))
    cotangent = noise_with(streams_of[3], (SEQS, LEN, F), 1.0, 16.0, ((0, 64), (2, 2)), (0, 2, 64, 4.0))
    w_gate = gaussian(streams_of[4], (D, F), D ** -0.5, 0.125, ((0, 4), (1, 2)))
    w_up = gaussian(streams_of[5], (D, F), D ** -0.5, 0.125, ((0, 4), (1, 2)))
    taps_gate = gaussian(streams_of[6], (TAPS, F), 0.6, 3.0)
    taps_up = gaussian(streams_of[7], (TAPS, F), 0.6, 3.0)
    return dict(inputs=inputs, pre_gate=pre_gate, pre_up=pre_up, cotangent=cotangent, w_gate=w_gate, w_up=w_up, taps_gate=taps_gate, taps_up=taps_up)


def causal_mix(signal, kernel):
    length = signal.shape[0]
    padded = jnp.pad(signal, ((2, 0), (0, 0)))
    return kernel[0] * padded[0:length] + kernel[1] * padded[1:length + 1] + kernel[2] * padded[2:length + 2]

def gated_hidden(gate_pre, up_pre, kernel_gate, kernel_up):
    return jax.nn.gelu(causal_mix(gate_pre, kernel_gate)) * causal_mix(up_pre, kernel_up)

def reference(inputs, pre_gate, pre_up, cotangent, w_gate, w_up, taps_gate, taps_up):
    kernel_gate = taps_gate.astype(jnp.float32)
    kernel_up = taps_up.astype(jnp.float32)
    block = F // N_TP

    def one_sequence(totals, item):
        rows, gate_seq, up_seq, back_seq = item
        _, pullback = jax.vjp(gated_hidden, gate_seq.astype(jnp.float32), up_seq.astype(jnp.float32), kernel_gate, kernel_up)
        back_gate, back_up, tap_gate, tap_up = pullback(back_seq.astype(jnp.float32))
        grad_gate = back_gate.astype(jnp.bfloat16)
        grad_up = back_up.astype(jnp.bfloat16)
        summed = jnp.zeros((rows.shape[0], rows.shape[1]), jnp.float32)
        for index in range(N_TP):
            lower = index * block
            partial_value = jnp.dot(grad_gate[:, lower:lower + block], w_gate[:, lower:lower + block].T, preferred_element_type=jnp.float32)
            partial_value = partial_value + jnp.dot(grad_up[:, lower:lower + block], w_up[:, lower:lower + block].T, preferred_element_type=jnp.float32)
            rounded = lax.optimization_barrier(partial_value.astype(jnp.bfloat16))
            summed = summed + rounded.astype(jnp.float32)
        new_totals = (totals[0] + jnp.dot(rows.T, grad_gate, preferred_element_type=jnp.float32), totals[1] + jnp.dot(rows.T, grad_up, preferred_element_type=jnp.float32), totals[2] + tap_gate, totals[3] + tap_up)
        return (new_totals, summed.astype(jnp.bfloat16))
    start = (jnp.zeros((D, F), jnp.float32), jnp.zeros((D, F), jnp.float32), jnp.zeros((TAPS, F), jnp.float32), jnp.zeros((TAPS, F), jnp.float32))
    totals, grad_inputs = lax.scan(one_sequence, start, (inputs, pre_gate, pre_up, cotangent))
    factor = float(TOKENS) ** (-0.5)
    return (grad_inputs, totals[0] * factor, totals[1] * factor, totals[2] * factor, totals[3] * factor)
```

```python
import functools

import jax
import jax.numpy as jnp
from jax import lax
from jax.experimental import pallas as pl
from jax.experimental.pallas import tpu as pltpu
from jax.sharding import PartitionSpec as P

F32 = jnp.float32
BF16 = jnp.bfloat16
MESH = pl.DeviceIdType.MESH

Y1, Y3, X1, X3, Z1, Z3 = range(6)
CYCLE = (X1, Z1, X3, Z3, Y1, Y3)
REP_CYCLE = (X1, Z1, X3, Z3)
GROUPS = ((0, 512), (512, 512), (1024, 384))
SUB = 32
PORTIONS = tuple((group, mat) for group in range(3) for mat in range(2))
ORDERS = tuple(tuple(CYCLE[(p + s) % 6] for s in range(6)) for p in range(6))
AG_START = (0, 1, 2, 3, 0, 2)
AG_ORDERS = tuple(tuple(REP_CYCLE[(a + t) % 4] for t in range(4)) for a in AG_START)
LEN = 768
HALF = 384
D = 2048
FC = 1408
W_PATHS = ((Y1, Y3), (Y3, Y1))
MASK = {Y1: 1, Y3: 3}


def recv_offset(stage):
    return 64 - 2 ** (6 - stage)


def kernel(
    x_hbm, gate_hbm, up_hbm, cot_hbm, wg_hbm, wu_hbm, kg_ref, ku_ref,
    gin_hbm, gwg_hbm, gwu_hbm, taps_hbm,
    xs, xt, act_g, act_u, act_c, ws_g, ws_u,
    g0, g1, g2, g3, g4, g5, r0, r1, r2, r3, r4, r5, a0, a1, a2, a3, a4, a5,
    stage_g, stage_u, tap, tap_in, tap_out, part, part_in,
    load_sem, rs_send, rs_recv, ag_send, ag_recv, wy_send, wy_recv, wf_send, wf_recv,
    t_send, t_recv, x_send, x_recv, o_send, o_recv, out_sem,
):
    gs, rs, ags = (g0, g1, g2, g3, g4, g5), (r0, r1, r2, r3, r4, r5), (a0, a1, a2, a3, a4, a5)
    ws = (ws_g, ws_u)
    acts = (act_g, act_u)
    stages = (stage_g, stage_u)
    rep, y, tp = lax.axis_index("rep"), lax.axis_index("fs"), lax.axis_index("tp")
    z, x = rep // 4, rep % 4

    def gray(c):
        return (c + c // 2) % 2, c // 2

    bits = gray(y) + gray(x) + gray(z)

    def flip1(c):
        return c + 1 - 2 * (c % 2)

    peers = (
        {"fs": flip1(y)}, {"fs": 3 - y},
        {"rep": z * 4 + flip1(x)}, {"rep": z * 4 + 3 - x},
        {"rep": flip1(z) * 4 + x}, {"rep": (3 - z) * 4 + x},
    )
    other_core = {"tp": 1 - tp}
    pending = []

    def remote(src, dst, send, recv, peer):
        return pltpu.make_async_remote_copy(
            src_ref=src, dst_ref=dst, send_sem=send, recv_sem=recv, device_id=peer, device_id_type=MESH
        )

    def send(copy):
        copy.start()
        pending.append(copy)

    loads = {}

    def load(name, src, dst):
        copy = pltpu.make_async_copy(src, dst, load_sem.at[len(loads)])
        copy.start()
        loads[name] = copy

    load("x", x_hbm, xs.at[tp])
    for mat, src in enumerate((wg_hbm, wu_hbm)):
        load("w" + str(mat), src, ws[mat].at[0])
    for group, (first, size) in enumerate(GROUPS):
        for name, src, dst in (("g", gate_hbm, act_g), ("u", up_hbm, act_u), ("c", cot_hbm, act_c)):
            load(name + str(group), src.at[:, pl.ds(first, size)], dst.at[:, pl.ds(first, size)])

    barrier = pltpu.get_barrier_semaphore()
    for peer in peers + (other_core,):
        pl.semaphore_signal(barrier, inc=1, device_id=peer, device_id_type=MESH)
    pl.semaphore_wait(barrier, 7)

    parity = (x % 2, z % 2)

    def wy_index(mat, mask, axis):
        return (mat * 3 + mask - 1) * 2 + axis

    def wy_copy(mat, src_mask, dim, axis):
        dst_mask = src_mask ^ MASK[dim]
        at = wy_index(mat, dst_mask, axis)
        return remote(
            ws[mat].at[src_mask, pl.ds(2 * axis, 2), parity[axis]],
            ws[mat].at[dst_mask, pl.ds(2 * axis, 2), parity[axis]],
            wy_send.at[at], wy_recv.at[at], peers[dim],
        )

    def wf_copy(mat, mask, link):
        at = (mat * 3 + mask - 1) * 4 + link
        half = ws[mat].at[mask, link, parity[link // 2]]
        return remote(half, half, wf_send.at[at], wf_recv.at[at], peers[2 + link])

    def w_own(mat, step, axis):
        send(wy_copy(mat, 0, W_PATHS[mat][step], axis))

    def w_wait_y(mat, step, relayed, axis):
        dim = W_PATHS[mat][step]
        src = MASK[W_PATHS[mat][0]] if relayed else 0
        wy_copy(mat, src, dim, axis).wait_recv()

    def w_relay(mat, axis):
        send(wy_copy(mat, MASK[W_PATHS[mat][0]], W_PATHS[mat][1], axis))

    def w_forward(mat, mask, axis):
        for link in (2 * axis, 2 * axis + 1):
            send(wf_copy(mat, mask, link))

    def w_done(mask):
        for mat in range(2):
            for link in range(4):
                wf_copy(mat, mask, link).wait_recv()

    row = lax.broadcasted_iota(jnp.int32, (LEN, 128), 0)

    def past(value, steps):
        return jnp.where(row >= steps, pltpu.roll(value, steps, 0), 0.0)

    def ahead(value, steps):
        return jnp.where(row < LEN - steps, pltpu.roll(value, LEN - steps, 0), 0.0)

    def elementwise(group):
        first, size = GROUPS[group]
        for name in ("g", "u", "c"):
            loads[name + str(group)].wait()

        def block(j, _):
            cols = pl.ds(pl.multiple_of(first + j * 128, 128), 128)
            tap_cols = pl.ds(pl.multiple_of(tp * FC + first + j * 128, 128), 128)
            kg_all = kg_ref[:, tap_cols].astype(F32)
            ku_all = ku_ref[:, tap_cols].astype(F32)
            kg = [kg_all[i : i + 1, :] for i in range(3)]
            ku = [ku_all[i : i + 1, :] for i in range(3)]
            gate = act_g[:, cols].astype(F32)
            gates = (past(gate, 2), past(gate, 1), gate)
            mixed_gate = kg[0] * gates[0] + kg[1] * gates[1] + kg[2] * gates[2]
            up = act_u[:, cols].astype(F32)
            ups = (past(up, 2), past(up, 1), up)
            mixed_up = ku[0] * ups[0] + ku[1] * ups[1] + ku[2] * ups[2]
            scale = (2.0 / 3.141592653589793) ** 0.5
            square = mixed_gate * mixed_gate
            bent = jnp.tanh(mixed_gate * (scale + (scale * 0.044715) * square))
            lift = 0.5 + 0.5 * bent
            slope = lift + mixed_gate * (1.0 - bent * bent) * (0.5 * scale + (1.5 * 0.044715 * scale) * square)
            cot = act_c[:, cols].astype(F32)
            back_up = cot * (mixed_gate * lift)
            back_gate = cot * mixed_up * slope
            dg = kg[2] * back_gate + kg[1] * ahead(back_gate, 1) + kg[0] * ahead(back_gate, 2)
            du = ku[2] * back_up + ku[1] * ahead(back_up, 1) + ku[0] * ahead(back_up, 2)
            act_g[:, cols] = dg.astype(BF16)
            act_u[:, cols] = du.astype(BF16)
            for i in range(3):
                tap[0, pl.ds(i, 1), cols] = jnp.sum(back_gate * gates[i], axis=0, keepdims=True)
                tap[0, pl.ds(3 + i, 1), cols] = jnp.sum(back_up * ups[i], axis=0, keepdims=True)
            return 0

        lax.fori_loop(0, size // 128, block, 0)

    def product(p):
        group, mat = PORTIONS[p]
        first, size = GROUPS[group]
        weights_at = {ORDERS[p][s]: 2 ** (5 - s) for s in range(6)}

        def block(yb, _):
            value = jnp.dot(
                xt[pl.ds(pl.multiple_of(yb * 512, 512), 512), :],
                acts[mat][:, pl.ds(first, size)],
                preferred_element_type=F32,
            ).astype(BF16)
            low, high = gray(yb)
            base = low * weights_at[Y1] + high * weights_at[Y3]
            for sub in range(16):
                at = sum(((sub >> k) & 1) * weights_at[2 + k] for k in range(4))
                gs[p][base + at] = value[sub * SUB : (sub + 1) * SUB, :]
            return 0

        lax.fori_loop(0, 4, block, 0)

    def base_of(p, stage):
        return sum(bits[ORDERS[p][s]] * 2 ** (5 - s) for s in range(stage))

    def rs_copy(p, stage):
        dim, count = ORDERS[p][stage], 2 ** (5 - stage)
        start = base_of(p, stage) + (1 - bits[dim]) * count
        at = p * 6 + stage
        return remote(
            gs[p].at[pl.ds(start, count)], rs[p].at[pl.ds(recv_offset(stage), count)],
            rs_send.at[at], rs_recv.at[at], peers[dim],
        )

    def ag_at(p):
        return sum(bits[dim] * 2**t for t, dim in enumerate(AG_ORDERS[p]))

    def ag_copy(p, step):
        count = 2**step
        held = ags[p].at[pl.ds((ag_at(p) // count) * count, count)]
        at = p * 4 + step
        return remote(held, held, ag_send.at[at], ag_recv.at[at], peers[AG_ORDERS[p][step]])

    def first_send(p):
        send(rs_copy(p, 0))

    def rs_step(p, stage):
        rs_copy(p, stage).wait_recv()
        start, count, offset = base_of(p, stage + 1), 2 ** (5 - stage), recv_offset(stage)

        def total(i):
            return (gs[p][start + i].astype(F32) + rs[p][offset + i].astype(F32)).astype(BF16)

        if stage == 5:
            ags[p][ag_at(p)] = total(0)
            send(ag_copy(p, 0))
            return

        def add(i, _):
            gs[p][start + i] = total(i)
            return 0

        lax.fori_loop(0, count, add, 0)
        send(rs_copy(p, stage + 1))

    def ag_step(p, step):
        ag_copy(p, step).wait_recv()
        if step < 3:
            send(ag_copy(p, step + 1))
            return
        group, mat = PORTIONS[p]
        first, size = GROUPS[group]
        for sub in range(16):
            at = sum(((sub >> (dim - 2)) & 1) * 2**t for t, dim in enumerate(AG_ORDERS[p]))
            stages[mat][pl.ds(sub * SUB, SUB), pl.ds(first, size)] = ags[p][at]

    def tap_copy(step):
        peer = peers[step] if step < 6 else other_core
        return remote(tap.at[step], tap_in.at[step], t_send.at[step], t_recv.at[step], peer)

    def tap_step(step):
        if step >= 0:
            tap_copy(step).wait_recv()
            tap[step + 1] = tap[step] + tap_in[step]
        send(tap_copy(step + 1))

    def back(mask):
        def block(n, _):
            def dot(mat):
                weights = ws[mat][mask, pl.ds(2 * n, 2)].reshape(256, FC)
                return lax.dot_general(
                    acts[mat][...], weights, (((1,), (1,)), ((), ())), preferred_element_type=F32
                )

            value = (dot(0) + dot(1)).astype(BF16)
            cols = pl.ds(pl.multiple_of(n * 256, 256), 256)
            part[mask, 0, :, cols] = value[:HALF]
            part[mask, 1, :, cols] = value[HALF:]
            return 0

        lax.fori_loop(0, 2, block, 0)
        send(part_copy(mask))

    def part_copy(mask):
        return remote(
            part.at[mask, 1 - tp], part_in.at[mask], o_send.at[mask], o_recv.at[mask], other_core
        )

    outs = []

    def finish(mask):
        part_copy(mask).wait_recv()
        part_in[mask] = (part[mask, tp].astype(F32) + part_in[mask].astype(F32)).astype(BF16)
        block = {0: y, 1: flip1(y), 2: (y + 2) % 4, 3: 3 - y}[mask]
        copy = pltpu.make_async_copy(
            part_in.at[mask],
            gin_hbm.at[:, pl.ds(pl.multiple_of(block * 512, 512), 512)],
            out_sem.at[len(outs)],
        )
        copy.start()
        outs.append(copy)

    def store(src, dst):
        copy = pltpu.make_async_copy(src, dst, out_sem.at[len(outs)])
        copy.start()
        outs.append(copy)

    loads["w0"].wait()
    loads["w1"].wait()
    for mat in range(2):
        for axis in range(2):
            w_own(mat, 0, axis)
    loads["x"].wait()
    x_copy = remote(xs.at[tp], xs.at[tp], x_send.at[0], x_recv.at[0], other_core)
    send(x_copy)
    tap[0] = jnp.zeros((8, FC), F32)

    elementwise(0)
    x_copy.wait_recv()

    def turn(c, _):
        cols = pl.ds(pl.multiple_of(c * 128, 128), 128)
        for h in range(2):
            xt[cols, pl.ds(h * HALF, HALF)] = xs[h, :, cols].T
        return 0

    lax.fori_loop(0, D // 128, turn, 0)
    product(0)
    first_send(0)
    product(1)
    first_send(1)
    elementwise(1)
    product(2)
    first_send(2)
    product(3)
    first_send(3)
    for axis in range(2):
        for mat in range(2):
            w_own(mat, 1, axis)
    elementwise(2)
    product(4)
    first_send(4)
    product(5)
    first_send(5)
    tap_step(-1)
    for axis in range(2):
        for mat in range(2):
            w_wait_y(mat, 0, False, axis)
            w_relay(mat, axis)
    back(0)
    rs_step(0, 0)
    rs_step(1, 0)
    for mat in range(2):
        for axis in range(2):
            w_forward(mat, MASK[W_PATHS[mat][0]], axis)
    rs_step(2, 0)
    rs_step(3, 0)
    tap_step(0)
    finish(0)
    rs_step(0, 1)
    rs_step(1, 1)
    rs_step(4, 0)
    rs_step(5, 0)
    for mat in range(2):
        for axis in range(2):
            w_wait_y(mat, 1, False, axis)
            w_forward(mat, MASK[W_PATHS[mat][1]], axis)
    tap_step(1)
    for p in range(4):
        rs_step(p, 2 if p < 2 else 1)
    rs_step(4, 1)
    rs_step(5, 1)
    tap_step(2)
    for p in range(4):
        rs_step(p, 3 if p < 2 else 2)
    rs_step(4, 2)
    rs_step(5, 2)
    tap_step(3)
    for p in range(4):
        rs_step(p, 4 if p < 2 else 3)
    rs_step(4, 3)
    rs_step(5, 3)
    tap_step(4)
    for p in range(4):
        rs_step(p, 5 if p < 2 else 4)
    rs_step(4, 4)
    rs_step(5, 4)
    for mat in range(2):
        for axis in range(2):
            w_wait_y(mat, 1, True, axis)
            w_forward(mat, 2, axis)
    rs_step(2, 5)
    rs_step(3, 5)
    rs_step(4, 5)
    rs_step(5, 5)
    tap_step(5)
    for step in range(3):
        for p in range(6):
            ag_step(p, step)
    w_done(1)
    back(1)
    w_done(3)
    back(3)
    finish(1)
    finish(3)
    for p in range(6):
        ag_step(p, 3)
    store(stage_g, gwg_hbm)
    store(stage_u, gwu_hbm)
    w_done(2)
    back(2)
    tap_copy(6).wait_recv()
    tap_out[tp] = tap[6]
    tap_out[1 - tp] = tap_in[6]
    store(tap_out, taps_hbm)
    finish(2)
    for copy in pending:
        copy.wait_send()
    for copy in outs:
        copy.wait()


def fused(x, gate, up, cot, wg, wu, kg, ku):
    sizes = [GROUPS[group][1] for group, _ in PORTIONS]
    any_space = pl.BlockSpec(memory_space=pl.ANY)
    in_vmem = pl.BlockSpec(memory_space=pltpu.VMEM)
    dma = pltpu.SemaphoreType.DMA
    return pl.pallas_call(
        kernel,
        in_specs=[any_space] * 6 + [in_vmem] * 2,
        out_specs=[any_space] * 4,
        out_shape=[
            jax.ShapeDtypeStruct((HALF, D), BF16),
            jax.ShapeDtypeStruct((512, FC), BF16),
            jax.ShapeDtypeStruct((512, FC), BF16),
            jax.ShapeDtypeStruct((2, 8, FC), F32),
        ],
        scratch_shapes=[
            pltpu.VMEM((2, HALF, D), BF16),
            pltpu.VMEM((D, LEN), BF16),
            pltpu.VMEM((LEN, FC), BF16),
            pltpu.VMEM((LEN, FC), BF16),
            pltpu.VMEM((LEN, FC), BF16),
            pltpu.VMEM((4, 4, 2, 64, FC), BF16),
            pltpu.VMEM((4, 4, 2, 64, FC), BF16),
        ]
        + [pltpu.VMEM((64, SUB, size), BF16) for size in sizes]
        + [pltpu.VMEM((63, SUB, size), BF16) for size in sizes]
        + [pltpu.VMEM((16, SUB, size), BF16) for size in sizes]
        + [
            pltpu.VMEM((512, FC), BF16),
            pltpu.VMEM((512, FC), BF16),
            pltpu.VMEM((7, 8, FC), F32),
            pltpu.VMEM((7, 8, FC), F32),
            pltpu.VMEM((2, 8, FC), F32),
            pltpu.VMEM((4, 2, HALF, 512), BF16),
            pltpu.VMEM((4, HALF, 512), BF16),
            dma((12,)), dma((36,)), dma((36,)), dma((24,)), dma((24,)),
            dma((12,)), dma((12,)), dma((24,)), dma((24,)),
            dma((7,)), dma((7,)), dma((1,)), dma((1,)), dma((4,)), dma((4,)), dma((7,)),
        ],
        compiler_params=pltpu.CompilerParams(
            collective_id=0, has_side_effects=True, vmem_limit_bytes=67043328
        ),
        cost_estimate=pl.CostEstimate(flops=18 * 10**9, bytes_accessed=20 * 2**20, transcendentals=10**6),
    )(x, gate, up, cot, wg, wu, kg, ku)


def per_device(inputs, pre_gate, pre_up, cotangent, w_gate, w_up, taps_gate, taps_up):
    count = LEN * lax.axis_size("rep") * lax.axis_size("fs")
    factor = float(count) ** (-0.5)
    grad_inputs, grad_gate, grad_up, taps = fused(
        inputs[0], pre_gate[0], pre_up[0], cotangent[0],
        w_gate.reshape(4, 2, 64, FC), w_up.reshape(4, 2, 64, FC), taps_gate, taps_up,
    )
    taps = factor * jnp.concatenate([taps[0], taps[1]], axis=1)
    return (
        grad_inputs[None],
        grad_gate.astype(F32) * factor,
        grad_up.astype(F32) * factor,
        taps[:3],
        taps[3:6],
    )


def solution(mesh):
    placed = (
        P(("rep", "fs"), "tp", None),
        P(("rep", "fs"), None, "tp"),
        P(("rep", "fs"), None, "tp"),
        P(("rep", "fs"), None, "tp"),
        P("fs", "tp"),
        P("fs", "tp"),
        P(),
        P(),
    )
    return jax.shard_map(
        per_device,
        mesh=mesh,
        in_specs=placed,
        out_specs=(P(("rep", "fs"), "tp", None), P("fs", "tp"), P("fs", "tp"), P(), P()),
        check_vma=False,
    )
```

```python
import functools

import jax
import jax.numpy as jnp
from jax import lax
from jax.experimental import pallas as pl
from jax.experimental.pallas import tpu as pltpu
from jax.sharding import PartitionSpec as P

F32 = jnp.float32
BF16 = jnp.bfloat16
MESH = pl.DeviceIdType.MESH

Y1, Y3, X1, X3, Z1, Z3 = range(6)
CYCLE = (X1, Z1, X3, Z3, Y1, Y3)
REP_CYCLE = (X1, Z1, X3, Z3)
GROUPS = ((0, 512), (512, 512), (1024, 384))
SPLIT = 2
SUB = 32
ROWS = SUB // SPLIT
PORTIONS = tuple((group, mat, h) for group in range(3) for mat in range(2) for h in range(SPLIT))
COUNT = len(PORTIONS)
GROUP_ORDER = (0, 2, 1)
ORDERS = (
    (X1, Z1, X3, Z3, Y1, Y3), (Z1, X1, Y1, Z3, Y3, X3), (Z3, Y1, Y3, X1, Z1, X3), (X3, Z3, X1, Y3, Y1, Z1),
    (X3, Z3, Y1, Y3, X1, Z1), (X1, Z1, X3, Z3, Y1, Y3), (Z3, Y1, Z1, X1, X3, Y3), (Z1, X3, Z3, Y1, X1, Y3),
    (Y1, Y3, X1, Z1, X3, Z3), (Y3, X1, Z1, Y1, Z3, X3), (Y1, Y3, Z1, X1, X3, Z3), (Y3, X3, Z1, Z3, X1, Y1),
)
AG_ORDERS = (
    (X1, X3, Z1, Z3), (X1, Z3, Z1, X3), (Z3, X3, Z1, X1), (Z1, X1, Z3, X3), (X3, Z3, Z1, X1),
    (Z3, Z1, X1, X3), (Z3, X3, X1, Z1), (X1, Z1, Z3, X3), (X3, Z1, Z3, X1), (Z3, X3, X1, Z1),
    (Z1, X3, Z3, X1), (Z1, Z3, X1, X3),
)
LEN = 768
HALF = 384
D = 2048
FC = 1408
W_PATHS = ((Y1, Y3), (Y3, Y1))
MASK = {Y1: 1, Y3: 3}


def recv_offset(stage):
    return 64 - 2 ** (6 - stage)


START, ELEM, TURN, PROD, RS, AG, WY, WF, TAP, BACK, FIN = range(11)
NAMES = ("start", "elem", "turn", "prod", "rs", "ag", "wy", "wf", "tap", "back", "fin")
SCHEDULE = (
    (ELEM, 0, 0, 2), (START,), (WY, 0, 0, Y1, 0), (WY, 1, 0, Y3, 0), (ELEM, 0, 2, 4), (WY, 0, 0, Y1, 1),
    (WY, 1, 0, Y3, 1), (TURN,), (PROD, 0, 0), (WY, 0, 0, Y1, 2), (WY, 1, 0, Y3, 2), (PROD, 0, 1),
    (WY, 0, 0, Y1, 3), (WY, 1, 0, Y3, 3), (ELEM, 2, 0, 2), (ELEM, 2, 2, 3), (PROD, 2, 0), (PROD, 2, 1),
    (ELEM, 1, 0, 2), (WF, 0, 1, 0), (WF, 0, 1, 2), (ELEM, 1, 2, 4), (WF, 0, 1, 1), (WF, 0, 1, 3),
    (PROD, 1, 0), (TAP, -1), (WF, 1, 3, 2), (PROD, 1, 1), (RS, 1, 0), (RS, 3, 0), (RS, 2, 0), (RS, 0, 0),
    (RS, 8, 0), (RS, 9, 0), (BACK, 0), (FIN, 0), (RS, 10, 0), (WF, 1, 3, 1), (RS, 11, 0), (RS, 5, 0),
    (WY, 1, 3, Y1, 0), (TAP, 0), (RS, 4, 0), (RS, 6, 0), (RS, 8, 1), (WY, 0, 1, Y3, 0), (RS, 7, 0),
    (RS, 2, 1), (RS, 1, 1), (RS, 10, 1), (RS, 3, 1), (RS, 0, 1), (WF, 1, 3, 3), (RS, 9, 1), (WY, 0, 1, Y3, 1),
    (RS, 11, 1), (TAP, 1), (WF, 1, 3, 0), (RS, 8, 2), (WY, 1, 3, Y1, 1), (RS, 4, 1), (WY, 0, 1, Y3, 2),
    (RS, 6, 1), (RS, 2, 2), (RS, 3, 2), (RS, 5, 1), (RS, 7, 1), (WF, 0, 2, 0), (RS, 1, 2), (RS, 10, 2),
    (WF, 0, 2, 1), (TAP, 2), (RS, 0, 2), (RS, 9, 2), (WY, 0, 1, Y3, 3), (WY, 1, 3, Y1, 2), (RS, 2, 3),
    (RS, 7, 2), (RS, 11, 2), (RS, 5, 2), (WF, 1, 2, 0), (WF, 0, 2, 2), (RS, 1, 3), (WF, 1, 2, 1), (RS, 8, 3),
    (RS, 3, 3), (RS, 0, 3), (RS, 4, 2), (RS, 11, 3), (RS, 9, 3), (RS, 6, 2), (WY, 0, 0, Y3, 0), (RS, 10, 3),
    (RS, 2, 4), (RS, 5, 3), (WF, 0, 2, 3), (RS, 9, 4), (RS, 1, 4), (WY, 1, 3, Y1, 3), (WF, 1, 2, 2),
    (WY, 0, 0, Y3, 1), (TAP, 3), (RS, 4, 3), (RS, 7, 3), (RS, 11, 4), (RS, 8, 4), (RS, 3, 4), (RS, 10, 4),
    (RS, 0, 4), (RS, 6, 3), (RS, 2, 5), (RS, 9, 5), (RS, 5, 4), (RS, 1, 5), (RS, 4, 4), (WY, 1, 0, Y1, 0),
    (RS, 7, 4), (WF, 0, 3, 0), (RS, 8, 5), (RS, 10, 5), (AG, 2, 0), (WY, 0, 0, Y3, 2), (AG, 9, 0), (RS, 6, 4),
    (AG, 1, 0), (AG, 8, 0), (RS, 3, 5), (WF, 1, 2, 3), (WY, 1, 0, Y1, 1), (RS, 4, 5), (RS, 11, 5),
    (AG, 10, 0), (AG, 2, 1), (WF, 0, 3, 1), (AG, 9, 1), (RS, 0, 5), (AG, 1, 1), (RS, 5, 5), (RS, 7, 5),
    (WY, 0, 0, Y3, 3), (AG, 8, 1), (TAP, 4), (AG, 4, 0), (AG, 3, 0), (AG, 11, 0), (AG, 10, 1),
    (WY, 1, 0, Y1, 2), (WF, 1, 1, 0), (AG, 2, 2), (AG, 9, 2), (AG, 0, 0), (AG, 7, 0), (AG, 1, 2), (BACK, 2),
    (WY, 1, 0, Y1, 3), (WF, 1, 1, 1), (WF, 0, 3, 2), (RS, 6, 5), (AG, 5, 0), (AG, 0, 1), (AG, 3, 1),
    (AG, 8, 2), (AG, 9, 3), (AG, 4, 1), (AG, 7, 1), (AG, 11, 1), (WF, 0, 3, 3), (FIN, 2), (AG, 10, 2),
    (AG, 1, 3), (AG, 6, 0), (TAP, 5), (AG, 3, 2), (AG, 2, 3), (AG, 7, 2), (WF, 1, 1, 2), (AG, 8, 3),
    (AG, 6, 1), (AG, 5, 1), (WF, 1, 1, 3), (AG, 11, 2), (AG, 0, 2), (BACK, 3), (AG, 4, 2), (AG, 6, 2),
    (AG, 3, 3), (AG, 10, 3), (AG, 5, 2), (AG, 7, 3), (BACK, 1), (FIN, 3), (AG, 0, 3), (AG, 11, 3), (AG, 4, 3),
    (AG, 6, 3), (AG, 5, 3), (FIN, 1),
)


def kernel(
    x_hbm, gate_hbm, up_hbm, cot_hbm, wg_hbm, wu_hbm, kg_ref, ku_ref,
    gin_hbm, gwg_hbm, gwu_hbm, taps_hbm,
    xs, xt, act_g, act_u, act_c, ws_g, ws_u,
    *scratch,
):
    gs, rs, ags = (scratch[i * COUNT : (i + 1) * COUNT] for i in range(3))
    (
        stage_g, stage_u, tap, tap_in, tap_out, part, part_in,
        load_sem, rs_send, rs_recv, ag_send, ag_recv, wy_send, wy_recv, wf_send, wf_recv,
        t_send, t_recv, x_send, x_recv, o_send, o_recv, out_sem,
    ) = scratch[3 * COUNT :]
    ws = (ws_g, ws_u)
    acts = (act_g, act_u)
    stages = (stage_g, stage_u)
    rep, y, tp = lax.axis_index("rep"), lax.axis_index("fs"), lax.axis_index("tp")
    z, x = rep // 4, rep % 4

    def gray(c):
        return (c + c // 2) % 2, c // 2

    bits = gray(y) + gray(x) + gray(z)

    def flip1(c):
        return c + 1 - 2 * (c % 2)

    peers = (
        {"fs": flip1(y)}, {"fs": 3 - y},
        {"rep": z * 4 + flip1(x)}, {"rep": z * 4 + 3 - x},
        {"rep": flip1(z) * 4 + x}, {"rep": (3 - z) * 4 + x},
    )
    other_core = {"tp": 1 - tp}
    pending = []

    def remote(src, dst, send, recv, peer):
        return pltpu.make_async_remote_copy(
            src_ref=src, dst_ref=dst, send_sem=send, recv_sem=recv, device_id=peer, device_id_type=MESH
        )

    def send(copy):
        copy.start()
        pending.append(copy)

    loads = {}

    def load(name, src, dst):
        copy = pltpu.make_async_copy(src, dst, load_sem.at[len(loads)])
        copy.start()
        loads[name] = copy

    def load_group(group):
        first, size = GROUPS[group]
        for name, src, dst in (("g", gate_hbm, act_g), ("u", up_hbm, act_u), ("c", cot_hbm, act_c)):
            load(name + str(group), src.at[:, pl.ds(first, size)], dst.at[:, pl.ds(first, size)])

    barrier = pltpu.get_barrier_semaphore()
    for peer in peers + (other_core,):
        pl.semaphore_signal(barrier, inc=1, device_id=peer, device_id_type=MESH)
    load_group(GROUP_ORDER[0])
    load("x", x_hbm, xs.at[tp])
    for mat, src in enumerate((wg_hbm, wu_hbm)):
        load("w" + str(mat), src, ws[mat].at[0])
    load_group(GROUP_ORDER[1])
    load_group(GROUP_ORDER[2])
    tap[0] = jnp.zeros((8, FC), F32)

    parity = (x % 2, z % 2)

    def wy_copy(mat, src_mask, dim, link):
        dst_mask = src_mask ^ MASK[dim]
        at = (mat * 3 + dst_mask - 1) * 4 + link
        half = parity[link // 2]
        return remote(
            ws[mat].at[src_mask, link, half], ws[mat].at[dst_mask, link, half],
            wy_send.at[at], wy_recv.at[at], peers[dim],
        )

    def wf_copy(mat, mask, link):
        at = (mat * 3 + mask - 1) * 4 + link
        half = ws[mat].at[mask, link, parity[link // 2]]
        return remote(half, half, wf_send.at[at], wf_recv.at[at], peers[2 + link])

    waited = set()

    def wy_wait(mat, mask, link):
        first, second = W_PATHS[mat]
        dim, src = {MASK[first]: (first, 0), MASK[second]: (second, 0), 2: (second, MASK[first])}[mask]
        if (mat, mask, link) not in waited:
            waited.add((mat, mask, link))
            wy_copy(mat, src, dim, link).wait_recv()

    def wy_step(mat, src_mask, dim, link):
        if src_mask:
            wy_wait(mat, src_mask, link)
        send(wy_copy(mat, src_mask, dim, link))

    def wf_step(mat, mask, link):
        wy_wait(mat, mask, link)
        send(wf_copy(mat, mask, link))

    row = lax.broadcasted_iota(jnp.int32, (LEN, 128), 0)

    def past(value, steps):
        return jnp.where(row >= steps, pltpu.roll(value, steps, 0), 0.0)

    def ahead(value, steps):
        return jnp.where(row < LEN - steps, pltpu.roll(value, LEN - steps, 0), 0.0)

    def elementwise(group, begin, end):
        first, size = GROUPS[group]
        if begin == 0:
            for name in ("g", "u", "c"):
                loads[name + str(group)].wait()

        def block(j, _):
            cols = pl.ds(pl.multiple_of(first + j * 128, 128), 128)
            tap_cols = pl.ds(pl.multiple_of(tp * FC + first + j * 128, 128), 128)
            kg_all = kg_ref[:, tap_cols].astype(F32)
            ku_all = ku_ref[:, tap_cols].astype(F32)
            kg = [kg_all[i : i + 1, :] for i in range(3)]
            ku = [ku_all[i : i + 1, :] for i in range(3)]
            gate = act_g[:, cols].astype(F32)
            gates = (past(gate, 2), past(gate, 1), gate)
            mixed_gate = kg[0] * gates[0] + kg[1] * gates[1] + kg[2] * gates[2]
            up = act_u[:, cols].astype(F32)
            ups = (past(up, 2), past(up, 1), up)
            mixed_up = ku[0] * ups[0] + ku[1] * ups[1] + ku[2] * ups[2]
            scale = (2.0 / 3.141592653589793) ** 0.5
            square = mixed_gate * mixed_gate
            bent = jnp.tanh(mixed_gate * (scale + (scale * 0.044715) * square))
            lift = 0.5 + 0.5 * bent
            slope = lift + mixed_gate * (1.0 - bent * bent) * (0.5 * scale + (1.5 * 0.044715 * scale) * square)
            cot = act_c[:, cols].astype(F32)
            back_up = cot * (mixed_gate * lift)
            back_gate = cot * mixed_up * slope
            dg = kg[2] * back_gate + kg[1] * ahead(back_gate, 1) + kg[0] * ahead(back_gate, 2)
            du = ku[2] * back_up + ku[1] * ahead(back_up, 1) + ku[0] * ahead(back_up, 2)
            act_g[:, cols] = dg.astype(BF16)
            act_u[:, cols] = du.astype(BF16)
            for i in range(3):
                tap[0, pl.ds(i, 1), cols] = jnp.sum(back_gate * gates[i], axis=0, keepdims=True)
                tap[0, pl.ds(3 + i, 1), cols] = jnp.sum(back_up * ups[i], axis=0, keepdims=True)
            return 0

        lax.fori_loop(begin, end, block, 0)

    def product(group, mat):
        first, size = GROUPS[group]
        mine = [p for p in range(COUNT) if PORTIONS[p][:2] == (group, mat)]
        places = [{ORDERS[p][s]: 2 ** (5 - s) for s in range(6)} for p in mine]

        def block(yb, _):
            value = jnp.dot(
                xt[pl.ds(pl.multiple_of(yb * 512, 512), 512), :],
                acts[mat][:, pl.ds(first, size)],
                preferred_element_type=F32,
            ).astype(BF16)
            low, high = gray(yb)
            for h, p in enumerate(mine):
                place = places[h]
                base = low * place[Y1] + high * place[Y3]
                for sub in range(16):
                    at = sum(((sub >> k) & 1) * place[2 + k] for k in range(4))
                    row_at = sub * SUB + h * ROWS
                    gs[p][base + at] = value[row_at : row_at + ROWS, :]
            return 0

        lax.fori_loop(0, 4, block, 0)
        for p in mine:
            send(rs_copy(p, 0))

    def base_of(p, stage):
        return sum(bits[ORDERS[p][s]] * 2 ** (5 - s) for s in range(stage))

    def rs_copy(p, stage):
        dim, count = ORDERS[p][stage], 2 ** (5 - stage)
        start = base_of(p, stage) + (1 - bits[dim]) * count
        at = p * 6 + stage
        return remote(
            gs[p].at[pl.ds(start, count)], rs[p].at[pl.ds(recv_offset(stage), count)],
            rs_send.at[at], rs_recv.at[at], peers[dim],
        )

    def ag_at(p):
        return sum(bits[dim] * 2**t for t, dim in enumerate(AG_ORDERS[p]))

    def ag_copy(p, step):
        count = 2**step
        held = ags[p].at[pl.ds((ag_at(p) // count) * count, count)]
        at = p * 4 + step
        return remote(held, held, ag_send.at[at], ag_recv.at[at], peers[AG_ORDERS[p][step]])

    def rs_step(p, stage):
        rs_copy(p, stage).wait_recv()
        start, count, offset = base_of(p, stage + 1), 2 ** (5 - stage), recv_offset(stage)

        def total(i):
            return (gs[p][start + i].astype(F32) + rs[p][offset + i].astype(F32)).astype(BF16)

        if stage == 5:
            ags[p][ag_at(p)] = total(0)
            send(ag_copy(p, 0))
            return

        def add(i, _):
            gs[p][start + i] = total(i)
            return 0

        lax.fori_loop(0, count, add, 0)
        send(rs_copy(p, stage + 1))

    def ag_step(p, step):
        ag_copy(p, step).wait_recv()
        if step < 3:
            send(ag_copy(p, step + 1))
            return
        group, mat, h = PORTIONS[p]
        first, size = GROUPS[group]
        for sub in range(16):
            at = sum(((sub >> (dim - 2)) & 1) * 2**t for t, dim in enumerate(AG_ORDERS[p]))
            stages[mat][pl.ds(sub * SUB + h * ROWS, ROWS), pl.ds(first, size)] = ags[p][at]

    def tap_copy(step):
        peer = peers[step] if step < 6 else other_core
        return remote(tap.at[step], tap_in.at[step], t_send.at[step], t_recv.at[step], peer)

    def tap_step(step):
        if step >= 0:
            tap_copy(step).wait_recv()
            tap[step + 1] = tap[step] + tap_in[step]
        send(tap_copy(step + 1))

    def back(mask):
        for mat in range(2):
            for link in range(4):
                if mask:
                    wy_wait(mat, mask, link)
                    wf_copy(mat, mask, link).wait_recv()

        def block(n, _):
            def dot(mat):
                weights = ws[mat][mask, pl.ds(2 * n, 2)].reshape(256, FC)
                return lax.dot_general(
                    acts[mat][...], weights, (((1,), (1,)), ((), ())), preferred_element_type=F32
                )

            value = (dot(0) + dot(1)).astype(BF16)
            cols = pl.ds(pl.multiple_of(n * 256, 256), 256)
            part[mask, 0, :, cols] = value[:HALF]
            part[mask, 1, :, cols] = value[HALF:]
            return 0

        lax.fori_loop(0, 2, block, 0)
        send(part_copy(mask))

    def part_copy(mask):
        return remote(
            part.at[mask, 1 - tp], part_in.at[mask], o_send.at[mask], o_recv.at[mask], other_core
        )

    outs = []

    def finish(mask):
        part_copy(mask).wait_recv()
        part_in[mask] = (part[mask, tp].astype(F32) + part_in[mask].astype(F32)).astype(BF16)
        block = {0: y, 1: flip1(y), 2: (y + 2) % 4, 3: 3 - y}[mask]
        copy = pltpu.make_async_copy(
            part_in.at[mask],
            gin_hbm.at[:, pl.ds(pl.multiple_of(block * 512, 512), 512)],
            out_sem.at[len(outs)],
        )
        copy.start()
        outs.append(copy)

    def store(src, dst):
        copy = pltpu.make_async_copy(src, dst, out_sem.at[len(outs)])
        copy.start()
        outs.append(copy)

    def turn():
        x_copy.wait_recv()

        def block(c, _):
            cols = pl.ds(pl.multiple_of(c * 128, 128), 128)
            for h in range(2):
                xt[cols, pl.ds(h * HALF, HALF)] = xs[h, :, cols].T
            return 0

        lax.fori_loop(0, D // 128, block, 0)

    def start():
        pl.semaphore_wait(barrier, 7)
        loads["x"].wait()
        send(x_copy)
        loads["w0"].wait()
        loads["w1"].wait()

    x_copy = remote(xs.at[tp], xs.at[tp], x_send.at[0], x_recv.at[0], other_core)
    run = {
        START: start, ELEM: elementwise, TURN: turn, PROD: product, RS: rs_step, AG: ag_step,
        WY: wy_step, WF: wf_step, TAP: tap_step, BACK: back, FIN: finish,
    }
    for op, *numbers in SCHEDULE:
        with jax.named_scope("_".join(str(n) for n in [NAMES[op]] + numbers)):
            run[op](*numbers)
    store(stage_g, gwg_hbm)
    store(stage_u, gwu_hbm)
    tap_copy(6).wait_recv()
    tap_out[tp] = tap[6]
    tap_out[1 - tp] = tap_in[6]
    store(tap_out, taps_hbm)
    for copy in pending:
        copy.wait_send()
    for copy in outs:
        copy.wait()


def fused(x, gate, up, cot, wg, wu, kg, ku):
    sizes = [GROUPS[group][1] for group, _, _ in PORTIONS]
    any_space = pl.BlockSpec(memory_space=pl.ANY)
    in_vmem = pl.BlockSpec(memory_space=pltpu.VMEM)
    dma = pltpu.SemaphoreType.DMA
    return pl.pallas_call(
        kernel,
        in_specs=[any_space] * 6 + [in_vmem] * 2,
        out_specs=[any_space] * 4,
        out_shape=[
            jax.ShapeDtypeStruct((HALF, D), BF16),
            jax.ShapeDtypeStruct((512, FC), BF16),
            jax.ShapeDtypeStruct((512, FC), BF16),
            jax.ShapeDtypeStruct((2, 8, FC), F32),
        ],
        scratch_shapes=[
            pltpu.VMEM((2, HALF, D), BF16),
            pltpu.VMEM((D, LEN), BF16),
            pltpu.VMEM((LEN, FC), BF16),
            pltpu.VMEM((LEN, FC), BF16),
            pltpu.VMEM((LEN, FC), BF16),
            pltpu.VMEM((4, 4, 2, 64, FC), BF16),
            pltpu.VMEM((4, 4, 2, 64, FC), BF16),
        ]
        + [pltpu.VMEM((64, ROWS, size), BF16) for size in sizes]
        + [pltpu.VMEM((63, ROWS, size), BF16) for size in sizes]
        + [pltpu.VMEM((16, ROWS, size), BF16) for size in sizes]
        + [
            pltpu.VMEM((512, FC), BF16),
            pltpu.VMEM((512, FC), BF16),
            pltpu.VMEM((7, 8, FC), F32),
            pltpu.VMEM((7, 8, FC), F32),
            pltpu.VMEM((2, 8, FC), F32),
            pltpu.VMEM((4, 2, HALF, 512), BF16),
            pltpu.VMEM((4, HALF, 512), BF16),
            dma((12,)), dma((6 * COUNT,)), dma((6 * COUNT,)), dma((4 * COUNT,)), dma((4 * COUNT,)),
            dma((24,)), dma((24,)), dma((24,)), dma((24,)),
            dma((7,)), dma((7,)), dma((1,)), dma((1,)), dma((4,)), dma((4,)), dma((7,)),
        ],
        compiler_params=pltpu.CompilerParams(
            collective_id=0, has_side_effects=True, vmem_limit_bytes=67043328
        ),
        cost_estimate=pl.CostEstimate(flops=18 * 10**9, bytes_accessed=20 * 2**20, transcendentals=10**6),
    )(x, gate, up, cot, wg, wu, kg, ku)


def per_device(inputs, pre_gate, pre_up, cotangent, w_gate, w_up, taps_gate, taps_up):
    count = LEN * lax.axis_size("rep") * lax.axis_size("fs")
    factor = float(count) ** (-0.5)
    grad_inputs, grad_gate, grad_up, taps = fused(
        inputs[0], pre_gate[0], pre_up[0], cotangent[0],
        w_gate.reshape(4, 2, 64, FC), w_up.reshape(4, 2, 64, FC), taps_gate, taps_up,
    )
    taps = factor * jnp.concatenate([taps[0], taps[1]], axis=1)
    return (
        grad_inputs[None],
        grad_gate.astype(F32) * factor,
        grad_up.astype(F32) * factor,
        taps[:3],
        taps[3:6],
    )


def solution(mesh):
    placed = (
        P(("rep", "fs"), "tp", None),
        P(("rep", "fs"), None, "tp"),
        P(("rep", "fs"), None, "tp"),
        P(("rep", "fs"), None, "tp"),
        P("fs", "tp"),
        P("fs", "tp"),
        P(),
        P(),
    )
    return jax.shard_map(
        per_device,
        mesh=mesh,
        in_specs=placed,
        out_specs=(P(("rep", "fs"), "tp", None), P("fs", "tp"), P("fs", "tp"), P(), P()),
        check_vma=False,
    )
```

```python
import functools

import jax
import jax.numpy as jnp
from jax import lax
from jax.experimental import pallas as pl
from jax.experimental.pallas import tpu as pltpu
from jax.sharding import PartitionSpec as P

F32 = jnp.float32
BF16 = jnp.bfloat16
MESH = pl.DeviceIdType.MESH

Y1, Y3, X1, X3, Z1, Z3 = range(6)
CYCLE = (X1, Z1, X3, Z3, Y1, Y3)
REP_CYCLE = (X1, Z1, X3, Z3)
GROUPS = ((0, 512), (512, 512), (1024, 384))
SPLIT = 2
SUB = 32
ROWS = SUB // SPLIT
PORTIONS = tuple((group, mat, h) for group in range(len(GROUPS)) for mat in range(2) for h in range(SPLIT))
COUNT = len(PORTIONS)
GROUP_ORDER = (0, 1, 2)
ORDERS = (
    (Z1, X1, X3, Y1, Z3, Y3), (Z3, X1, Y1, Y3, Z1, X3), (X1, Y3, Z3, Z1, X3, Y1), (X3, Z3, Z1, Y1, X1, Y3),
    (Y1, X1, Z1, Z3, Y3, X3), (X3, Z3, X1, Y1, Y3, Z1), (Z3, X3, Z1, Y3, Y1, X1), (X1, Y3, X3, Z1, Z3, Y1),
    (Z3, Z1, X1, Y3, X3, Y1), (Z1, X3, X1, Z3, Y3, Y1), (Y1, Z1, X3, X1, Y3, Z3), (Y3, Z1, X3, Z3, X1, Y1),
)
AG_ORDERS = (
    (X3, Z1, X1, Z3), (Z1, Z3, X3, X1), (X3, X1, Z3, Z1), (Z1, Z3, X3, X1), (Z3, X1, Z1, X3),
    (Z3, X3, X1, Z1), (Z3, X3, Z1, X1), (Z1, Z3, X1, X3), (X1, X3, Z1, Z3), (X1, Z1, Z3, X3),
    (Z1, X1, X3, Z3), (Z3, X3, X1, Z1),
)
DIRECT = ((0, 0), (1, 3))
LEN = 768
HALF = 384
D = 2048
FC = 1408
STEP = 1024
W_PATHS = ((Y1, Y3), (Y3, Y1))
MASK = {Y1: 1, Y3: 3}


def recv_offset(stage):
    return 64 - 2 ** (6 - stage)


START, ELEM, TURN, PROD, RS, AG, WY, WF, TAP, BACK, FIN = range(11)
NAMES = ("start", "elem", "turn", "prod", "rs", "ag", "wy", "wf", "tap", "back", "fin")
SCHEDULE = (
    (ELEM, 0, 0, 1), (TURN, 0), (START,), (WY, 0, 0, Y1, 2, 0), (WY, 1, 0, Y3, 1, 0), (ELEM, 0, 1, 4),
    (WY, 0, 0, Y1, 0, 0), (WY, 0, 0, Y3, 2, 0), (TURN, 1), (PROD, 0, 0), (WY, 0, 0, Y1, 3, 0),
    (WY, 1, 0, Y3, 3, 0), (WF, 1, 3, 1), (PROD, 0, 1), (ELEM, 1, 0, 2), (WY, 1, 0, Y1, 0, 0),
    (WY, 1, 0, Y3, 0, 0), (ELEM, 1, 2, 4), (PROD, 1, 0), (WY, 0, 0, Y3, 1, 0), (PROD, 1, 1), (ELEM, 2, 0, 1),
    (WF, 0, 1, 2), (ELEM, 2, 1, 3), (WY, 0, 0, Y3, 0, 0), (PROD, 2, 0), (TAP, -1), (PROD, 2, 1), (RS, 0, 0),
    (RS, 2, 0), (RS, 1, 0), (BACK, 0, 0), (RS, 3, 0), (BACK, 0, 1), (FIN, 0, 0), (FIN, 0, 1), (RS, 4, 0),
    (WF, 0, 3, 2), (RS, 6, 0), (RS, 9, 0), (TAP, 0), (RS, 7, 0), (RS, 11, 0), (WY, 1, 0, Y1, 1, 0),
    (RS, 5, 0), (RS, 10, 0), (WY, 0, 0, Y1, 1, 0), (RS, 0, 1), (RS, 2, 1), (RS, 8, 0), (RS, 11, 1),
    (RS, 6, 1), (WY, 1, 0, Y1, 2, 0), (WY, 1, 0, Y3, 2, 0), (TAP, 1), (RS, 1, 1), (RS, 10, 1), (RS, 9, 1),
    (RS, 3, 1), (RS, 7, 1), (WY, 0, 1, Y3, 1, 0), (RS, 0, 2), (RS, 8, 1), (RS, 11, 2), (RS, 4, 1),
    (WY, 1, 0, Y1, 3, 0), (WY, 0, 1, Y3, 2, 0), (RS, 5, 1), (WF, 0, 1, 3), (WF, 0, 1, 1), (RS, 6, 2),
    (RS, 10, 2), (RS, 1, 2), (RS, 9, 2), (RS, 0, 3), (RS, 2, 2), (TAP, 2), (WY, 1, 3, Y1, 0, 0), (RS, 3, 2),
    (RS, 11, 3), (RS, 7, 2), (RS, 8, 2), (WF, 0, 3, 1), (WF, 1, 3, 0), (WF, 1, 3, 2), (RS, 4, 2), (RS, 5, 2),
    (WY, 0, 0, Y3, 3, 0), (RS, 2, 3), (RS, 6, 3), (RS, 10, 3), (RS, 11, 4), (RS, 9, 3), (RS, 7, 3),
    (WF, 1, 1, 0), (RS, 0, 4), (RS, 1, 3), (WF, 0, 2, 1), (RS, 8, 3), (WF, 1, 1, 2), (RS, 4, 3),
    (WY, 1, 3, Y1, 1, 0), (TAP, 3), (RS, 3, 3), (RS, 7, 4), (RS, 5, 3), (RS, 2, 4), (RS, 1, 4), (RS, 6, 4),
    (WY, 0, 1, Y3, 0, 0), (RS, 11, 5), (WF, 1, 2, 0), (WF, 0, 3, 3), (WF, 1, 1, 1), (RS, 10, 4),
    (WF, 0, 2, 2), (RS, 9, 4), (RS, 0, 5), (WY, 1, 3, Y1, 2, 0), (RS, 4, 4), (AG, 11, 0), (RS, 3, 4),
    (RS, 5, 4), (RS, 6, 5), (RS, 8, 4), (RS, 1, 5), (WY, 0, 1, Y3, 3, 0), (RS, 7, 5), (RS, 2, 5), (RS, 9, 5),
    (WY, 1, 3, Y1, 3, 0), (WF, 1, 2, 1), (RS, 10, 5), (AG, 6, 0), (RS, 3, 5), (TAP, 4), (AG, 9, 0),
    (WY, 1, 0, Y3, 3, 1), (AG, 0, 0), (RS, 4, 5), (RS, 5, 5), (WF, 1, 2, 2), (AG, 11, 1), (RS, 8, 5),
    (AG, 1, 0), (AG, 2, 0), (AG, 7, 0), (AG, 10, 0), (WY, 0, 0, Y1, 0, 1), (AG, 3, 0), (AG, 9, 1), (AG, 4, 0),
    (AG, 0, 1), (WF, 0, 2, 3), (AG, 5, 0), (WY, 0, 0, Y3, 0, 1), (AG, 1, 1), (AG, 11, 2), (AG, 8, 0),
    (AG, 7, 1), (AG, 2, 1), (AG, 3, 1), (WY, 1, 0, Y1, 3, 1), (TAP, 5), (AG, 10, 1), (AG, 6, 1), (AG, 4, 1),
    (AG, 5, 1), (AG, 9, 2), (BACK, 3, 1), (AG, 0, 2), (AG, 1, 2), (AG, 8, 1), (WY, 0, 1, Y3, 0, 1),
    (BACK, 1, 0), (WY, 1, 3, Y1, 3, 1), (AG, 7, 2), (AG, 3, 2), (FIN, 3, 1), (AG, 11, 3), (AG, 6, 2),
    (AG, 5, 2), (BACK, 3, 0), (AG, 2, 2), (AG, 4, 2), (AG, 10, 2), (FIN, 1, 0), (BACK, 1, 1), (AG, 8, 2),
    (AG, 9, 3), (AG, 1, 3), (FIN, 3, 0), (AG, 0, 3), (BACK, 2, 0), (AG, 7, 3), (AG, 5, 3), (FIN, 1, 1),
    (AG, 3, 3), (BACK, 2, 1), (AG, 10, 3), (FIN, 2, 0), (AG, 4, 3), (AG, 2, 3), (AG, 8, 3), (AG, 6, 3),
    (FIN, 2, 1),
)


def kernel(
    x_hbm, gate_hbm, up_hbm, cot_hbm, wg_hbm, wu_hbm, kg_ref, ku_ref,
    gin_hbm, taps_hbm, *rest,
):
    sums, (xs, xt, act_g, act_u, act_c, ws_g, ws_u, *scratch) = rest[:COUNT], rest[COUNT:]
    gs, rs, ags = (scratch[i * COUNT : (i + 1) * COUNT] for i in range(3))
    (
        tap, tap_in, tap_out, part, part_in,
        load_sem, rs_send, rs_recv, ag_send, ag_recv, w_send, wy_recv, wf_recv,
        t_send, t_recv, x_send, x_recv, o_send, o_recv, out_sem, sum_sem,
    ) = scratch[3 * COUNT :]
    ws = (ws_g, ws_u)
    acts = (act_g, act_u)
    rep, y, tp = lax.axis_index("rep"), lax.axis_index("fs"), lax.axis_index("tp")
    z, x = rep // 4, rep % 4

    def gray(c):
        return (c + c // 2) % 2, c // 2

    bits = gray(y) + gray(x) + gray(z)

    def flip1(c):
        return c + 1 - 2 * (c % 2)

    peers = (
        {"fs": flip1(y)}, {"fs": 3 - y},
        {"rep": z * 4 + flip1(x)}, {"rep": z * 4 + 3 - x},
        {"rep": flip1(z) * 4 + x}, {"rep": (3 - z) * 4 + x},
    )
    other_core = {"tp": 1 - tp}

    def remote(src, dst, send, recv, peer):
        return pltpu.make_async_remote_copy(
            src_ref=src, dst_ref=dst, send_sem=send, recv_sem=recv, device_id=peer, device_id_type=MESH
        )

    def send(copy):
        copy.start()

    loads = {}

    def load(name, src, dst):
        copy = pltpu.make_async_copy(src, dst, load_sem.at[len(loads)])
        copy.start()
        loads[name] = copy

    def load_group(key, first, size):
        for name, src, dst in (("g", gate_hbm, act_g), ("u", up_hbm, act_u), ("c", cot_hbm, act_c)):
            load(name + str(key), src.at[:, pl.ds(first, size)], dst.at[:, pl.ds(first, size)])

    barrier = pltpu.get_barrier_semaphore()
    for peer in peers + (other_core,):
        pl.semaphore_signal(barrier, inc=1, device_id=peer, device_id_type=MESH)
    load_group("first", 0, 128)
    load_group(0, 128, GROUPS[0][1] - 128)
    load("x", x_hbm, xs.at[tp])
    for mat, src in enumerate((wg_hbm, wu_hbm)):
        load("w" + str(mat), src, ws[mat].at[0])
    for group in range(1, len(GROUPS)):
        load_group(group, *GROUPS[group])
    tap[0] = jnp.zeros((8, FC), F32)

    parity = (x % 2, z % 2)

    waited = set()

    def wy_copy(mat, src_mask, dim, link, far):
        dst_mask = src_mask ^ MASK[dim]
        at = (mat * 3 + dst_mask - 1) * 4 + link
        half = parity[link // 2]
        if far:
            at, half = 24 + DIRECT.index((mat, link)) * 3 + dst_mask - 1, 1 - half
        return remote(
            ws[mat].at[src_mask, link, half], ws[mat].at[dst_mask, link, half],
            w_send.at[mat], wy_recv.at[at], peers[dim],
        )

    def wf_copy(mat, mask, link):
        half = ws[mat].at[mask, link, parity[link // 2]]
        at = (mask - 1) * 2 + link // 2
        return remote(half, half, w_send.at[mat], wf_recv.at[at], peers[2 + link])

    def landed(ref, sem):
        pltpu.make_async_copy(ref, ref, sem).wait()

    def wf_wait(mask, n):
        count = 4 - sum(link // 2 == n for _, link in DIRECT)
        if count:
            landed(ws[0].at[pl.ds(0, count), 0, 0], wf_recv.at[(mask - 1) * 2 + n])

    def wy_wait(mat, mask, link, far):
        first, second = W_PATHS[mat]
        dim, src = {MASK[first]: (first, 0), MASK[second]: (second, 0), 2: (second, MASK[first])}[mask]
        if (mat, mask, link, far) not in waited:
            waited.add((mat, mask, link, far))
            wy_copy(mat, src, dim, link, far).wait_recv()

    def own_loaded(mat):
        if mat not in waited:
            waited.add(mat)
            loads["w" + str(mat)].wait()

    def wy_step(mat, src_mask, dim, link, far):
        if src_mask:
            wy_wait(mat, src_mask, link, far)
        else:
            own_loaded(mat)
        send(wy_copy(mat, src_mask, dim, link, far))

    def wf_step(mat, mask, link):
        wy_wait(mat, mask, link, 0)
        send(wf_copy(mat, mask, link))

    row = lax.broadcasted_iota(jnp.int32, (8, 128), 0)

    def past(value, steps):
        turned = pltpu.roll(value, steps, 0)
        return jnp.concatenate([jnp.where(row >= steps, turned[:8], 0.0), turned[8:]], axis=0)

    def ahead(value, steps):
        turned = pltpu.roll(value, LEN - steps, 0)
        return jnp.concatenate([turned[:-8], jnp.where(row < 8 - steps, turned[-8:], 0.0)], axis=0)

    def group_loaded(group):
        if ("group", group) not in waited:
            waited.add(("group", group))
            for name in ("g", "u", "c"):
                loads[name + str(group)].wait()

    def elementwise_block(first, j):
        cols = pl.ds(pl.multiple_of(first + j * 128, 128), 128)
        tap_cols = pl.ds(pl.multiple_of(tp * FC + first + j * 128, 128), 128)
        kg_all = kg_ref[:, tap_cols].astype(F32)
        ku_all = ku_ref[:, tap_cols].astype(F32)
        kg = [kg_all[i : i + 1, :] for i in range(3)]
        ku = [ku_all[i : i + 1, :] for i in range(3)]
        gate = act_g[:, cols].astype(F32)
        gates = (past(gate, 2), past(gate, 1), gate)
        mixed_gate = kg[0] * gates[0] + kg[1] * gates[1] + kg[2] * gates[2]
        up = act_u[:, cols].astype(F32)
        ups = (past(up, 2), past(up, 1), up)
        mixed_up = ku[0] * ups[0] + ku[1] * ups[1] + ku[2] * ups[2]
        scale = (2.0 / 3.141592653589793) ** 0.5
        square = mixed_gate * mixed_gate
        bent = jnp.tanh(mixed_gate * (scale + (scale * 0.044715) * square))
        lift = 0.5 + 0.5 * bent
        slope = lift + mixed_gate * (1.0 - bent * bent) * (0.5 * scale + (1.5 * 0.044715 * scale) * square)
        cot = act_c[:, cols].astype(F32)
        back_up = cot * (mixed_gate * lift)
        back_gate = cot * mixed_up * slope
        dg = kg[2] * back_gate + kg[1] * ahead(back_gate, 1) + kg[0] * ahead(back_gate, 2)
        du = ku[2] * back_up + ku[1] * ahead(back_up, 1) + ku[0] * ahead(back_up, 2)
        act_g[:, cols] = dg.astype(BF16)
        act_u[:, cols] = du.astype(BF16)
        for i in range(3):
            tap[0, pl.ds(i, 1), cols] = jnp.sum(back_gate * gates[i], axis=0, keepdims=True)
            tap[0, pl.ds(3 + i, 1), cols] = jnp.sum(back_up * ups[i], axis=0, keepdims=True)

    def elementwise(group, begin, end):
        if group == 0 and begin == 0:
            group_loaded("first")
            elementwise_block(0, 0)
            begin = 1
        group_loaded(group)

        def block(j, _):
            elementwise_block(GROUPS[group][0], j)
            return 0

        lax.fori_loop(begin, end, block, 0)

    def product_block(group, mat, step):
        first, size = GROUPS[group]
        value = jnp.dot(
            xt[pl.ds(pl.multiple_of(step * STEP, STEP), STEP), :],
            acts[mat][:, pl.ds(first, size)],
            preferred_element_type=F32,
        ).astype(BF16)
        for k in range(STEP // 512):
            low, high = gray(step * (STEP // 512) + k)
            for p in range(COUNT):
                if PORTIONS[p][:2] != (group, mat):
                    continue
                place = {ORDERS[p][s]: 2 ** (5 - s) for s in range(6)}
                base = low * place[Y1] + high * place[Y3]
                for sub in range(16):
                    at = sum(((sub >> i) & 1) * place[2 + i] for i in range(4))
                    row_at = k * 512 + sub * SUB + PORTIONS[p][2] * ROWS
                    gs[p][base + at] = value[row_at : row_at + ROWS, :]

    def product_done(group, mat):
        for p in range(COUNT):
            if PORTIONS[p][:2] == (group, mat):
                send(rs_copy(p, 0))

    def product(group, mat):
        def block(step, _):
            product_block(group, mat, step)
            return 0

        lax.fori_loop(0, D // STEP, block, 0)
        product_done(group, mat)

    def base_of(p, stage):
        return sum(bits[ORDERS[p][s]] * 2 ** (5 - s) for s in range(stage))

    def rs_copy(p, stage):
        dim, count = ORDERS[p][stage], 2 ** (5 - stage)
        start = base_of(p, stage) + (1 - bits[dim]) * count
        at = p * 6 + stage
        return remote(
            gs[p].at[pl.ds(start, count)], rs[p].at[pl.ds(recv_offset(stage), count)],
            rs_send.at[p], rs_recv.at[at], peers[dim],
        )

    def ag_at(p):
        return sum(bits[dim] * 2**t for t, dim in enumerate(AG_ORDERS[p]))

    def ag_copy(p, step):
        count = 2**step
        held = ags[p].at[pl.ds((ag_at(p) // count) * count, count)]
        at = p * 4 + step
        return remote(held, held, ag_send.at[p], ag_recv.at[at], peers[AG_ORDERS[p][step]])

    def rs_step(p, stage):
        rs_copy(p, stage).wait_recv()
        start, count, offset = base_of(p, stage + 1), 2 ** (5 - stage), recv_offset(stage)

        def total(i):
            return (gs[p][start + i].astype(F32) + rs[p][offset + i].astype(F32)).astype(BF16)

        if stage == 5:
            ags[p][ag_at(p)] = total(0)
            send(ag_copy(p, 0))
            return

        def add(i, _):
            gs[p][start + i] = total(i)
            return 0

        lax.fori_loop(0, count, add, 0)
        send(rs_copy(p, stage + 1))

    def ag_step(p, step):
        ag_copy(p, step).wait_recv()
        if step < 3:
            send(ag_copy(p, step + 1))
            return
        pltpu.make_async_copy(ags[p], sums[p], sum_sem.at[PORTIONS[p][0]]).start()

    def tap_copy(step):
        peer = peers[step] if step < 6 else other_core
        return remote(tap.at[step], tap_in.at[step], t_send.at[0], t_recv.at[step], peer)

    def tap_step(step):
        if step >= 0:
            tap_copy(step).wait_recv()
            tap[step + 1] = tap[step] + tap_in[step]
        send(tap_copy(step + 1))

    def back(mask, n):
        for mat in range(2):
            own_loaded(mat)
            for link in (2 * n, 2 * n + 1) if mask else ():
                wy_wait(mat, mask, link, 0)
                if (mat, link) in DIRECT:
                    wy_wait(mat, mask, link, 1)
        if mask:
            wf_wait(mask, n)

        def dot(mat):
            weights = ws[mat][mask, pl.ds(2 * n, 2)].reshape(256, FC)
            return lax.dot_general(
                acts[mat][...], weights, (((1,), (1,)), ((), ())), preferred_element_type=F32
            )

        value = (dot(0) + dot(1)).astype(BF16)
        part[mask, n, 0] = value[:HALF]
        part[mask, n, 1] = value[HALF:]
        send(part_copy(mask, n))

    def part_copy(mask, n):
        return remote(
            part.at[mask, n, 1 - tp], part_in.at[mask, n], o_send.at[0], o_recv.at[mask * 2 + n], other_core
        )

    def finish(mask, n):
        part_copy(mask, n).wait_recv()
        part_in[mask, n] = (part[mask, n, tp].astype(F32) + part_in[mask, n].astype(F32)).astype(BF16)
        block = {0: y, 1: flip1(y), 2: (y + 2) % 4, 3: 3 - y}[mask]
        cols = pl.ds(pl.multiple_of(block * 512 + n * 256, 256), 256)
        pltpu.make_async_copy(part_in.at[mask, n], gin_hbm.at[:, cols], out_sem.at[0]).start()

    def x_loaded():
        if "x" not in waited:
            waited.add("x")
            loads["x"].wait()

    def turn(second):
        if second:
            x_copy.wait_recv()
        else:
            x_loaded()
        which = 1 - tp if second else tp
        rows = pl.ds(pl.multiple_of(which * HALF, HALF), HALF)

        def block(c, _):
            cols = pl.ds(pl.multiple_of(c * 128, 128), 128)
            xt[cols, rows] = xs[which, :, cols].T
            return 0

        lax.fori_loop(0, D // 128, block, 0)

    def start():
        pl.semaphore_wait(barrier, 7)
        x_loaded()
        send(x_copy)

    x_copy = remote(xs.at[tp], xs.at[tp], x_send.at[0], x_recv.at[0], other_core)
    run = {
        START: start, ELEM: elementwise, TURN: turn, PROD: product, RS: rs_step, AG: ag_step,
        WY: wy_step, WF: wf_step, TAP: tap_step, BACK: back, FIN: finish,
    }
    for op, *numbers in SCHEDULE:
        with jax.named_scope("_".join(str(n) for n in [NAMES[op]] + numbers)):
            run[op](*numbers)
    with jax.named_scope("tail_taps"):
        tap_copy(6).wait_recv()
        tap_out[tp] = tap[6]
        tap_out[1 - tp] = tap_in[6]
        tap_store = pltpu.make_async_copy(tap_out, taps_hbm, out_sem.at[1])
        tap_store.start()
    with jax.named_scope("tail_sends"):
        for p in range(COUNT):
            landed(rs[p], rs_send.at[p])
            landed(ags[p].at[pl.ds(0, 15)], ag_send.at[p])
        for mat in range(2):
            landed(ws[mat].at[pl.ds(0, 3)], w_send.at[mat])
        landed(tap, t_send.at[0])
        landed(part_in, o_send.at[0])
        x_copy.wait_send()
    with jax.named_scope("tail_stores"):
        for group in range(len(GROUPS)):
            landed(gs[group * 2 * SPLIT].at[pl.ds(0, 32 * SPLIT)], sum_sem.at[group])
        landed(part_in, out_sem.at[0])
        tap_store.wait()


def fused(x, gate, up, cot, wg, wu, kg, ku):
    sizes = [GROUPS[group][1] for group, _, _ in PORTIONS]
    any_space = pl.BlockSpec(memory_space=pl.ANY)
    in_vmem = pl.BlockSpec(memory_space=pltpu.VMEM)
    dma = pltpu.SemaphoreType.DMA
    return pl.pallas_call(
        kernel,
        in_specs=[any_space] * 6 + [in_vmem] * 2,
        out_specs=[any_space] * (2 + COUNT),
        out_shape=[jax.ShapeDtypeStruct((HALF, D), BF16), jax.ShapeDtypeStruct((2, 8, FC), F32)]
        + [jax.ShapeDtypeStruct((16, ROWS, size), BF16) for size in sizes],
        scratch_shapes=[
            pltpu.VMEM((2, HALF, D), BF16),
            pltpu.VMEM((D, LEN), BF16),
            pltpu.VMEM((LEN, FC), BF16),
            pltpu.VMEM((LEN, FC), BF16),
            pltpu.VMEM((LEN, FC), BF16),
            pltpu.VMEM((4, 4, 2, 64, FC), BF16),
            pltpu.VMEM((4, 4, 2, 64, FC), BF16),
        ]
        + [pltpu.VMEM((64, ROWS, size), BF16) for size in sizes]
        + [pltpu.VMEM((63, ROWS, size), BF16) for size in sizes]
        + [pltpu.VMEM((16, ROWS, size), BF16) for size in sizes]
        + [
            pltpu.VMEM((7, 8, FC), F32),
            pltpu.VMEM((7, 8, FC), F32),
            pltpu.VMEM((2, 8, FC), F32),
            pltpu.VMEM((4, 2, 2, HALF, 256), BF16),
            pltpu.VMEM((4, 2, HALF, 256), BF16),
            dma((6 + 3 * len(GROUPS),)),
            dma((COUNT,)), dma((6 * COUNT,)), dma((COUNT,)), dma((4 * COUNT,)),
            dma((2,)), dma((24 + 3 * len(DIRECT),)), dma((6,)),
            dma((1,)), dma((7,)), dma((1,)), dma((1,)), dma((1,)), dma((8,)), dma((2,)), dma((len(GROUPS),)),
        ],
        compiler_params=pltpu.CompilerParams(
            collective_id=0, has_side_effects=True, vmem_limit_bytes=67043328
        ),
        cost_estimate=pl.CostEstimate(flops=18 * 10**9, bytes_accessed=20 * 2**20, transcendentals=10**6),
    )(x, gate, up, cot, wg, wu, kg, ku)


def finish_kernel(factor, gin_hbm, taps_ref, *rest):
    sums, rest = rest[:COUNT], rest[COUNT:]
    gin_out, gate_out, up_out, tap_gate, tap_up, gin, *rest = rest
    held, (wide_gate, wide_up, in_sem, out_sem) = rest[:COUNT], rest[COUNT:]
    wide, results = (wide_gate, wide_up), (gate_out, up_out)
    copies = [pltpu.make_async_copy(sums[p], held[p], in_sem.at[p]) for p in range(COUNT)]
    for copy in copies:
        copy.start()
    gin_in = pltpu.make_async_copy(gin_hbm, gin, in_sem.at[COUNT])
    gin_in.start()
    for i in range(2):
        cols = pl.ds(i * FC, FC)
        tap_gate[:, cols] = factor * taps_ref[i, :3, :]
        tap_up[:, cols] = factor * taps_ref[i, 3:6, :]
    outs = []
    for p in range(COUNT):
        with jax.named_scope("sum_wait_" + str(p)):
            copies[p].wait()
        group, mat, h = PORTIONS[p]
        first, size = GROUPS[group]
        for sub in range(16):
            at = sum(((sub >> (dim - 2)) & 1) * 2**t for t, dim in enumerate(AG_ORDERS[p]))
            rows = pl.ds(sub * SUB + h * ROWS, ROWS)
            wide[mat][rows, pl.ds(first, size)] = factor * held[p][at].astype(F32)
        if h == SPLIT - 1:
            cols = pl.ds(first, size)
            copy = pltpu.make_async_copy(wide[mat].at[:, cols], results[mat].at[:, cols], out_sem.at[len(outs)])
            copy.start()
            outs.append(copy)
    gin_in.wait()
    copy = pltpu.make_async_copy(gin, gin_out, out_sem.at[len(outs)])
    copy.start()
    with jax.named_scope("last_wait"):
        for copy in outs + [copy]:
            copy.wait()


def finished(factor, gin, taps, sums):
    any_space = pl.BlockSpec(memory_space=pl.ANY)
    in_vmem = pl.BlockSpec(memory_space=pltpu.VMEM)
    return pl.pallas_call(
        functools.partial(finish_kernel, factor),
        in_specs=[any_space, in_vmem] + [any_space] * COUNT,
        out_specs=[any_space] * 3 + [in_vmem] * 2,
        out_shape=[
            jax.ShapeDtypeStruct((HALF, D), BF16),
            jax.ShapeDtypeStruct((512, FC), F32),
            jax.ShapeDtypeStruct((512, FC), F32),
            jax.ShapeDtypeStruct((3, 2 * FC), F32),
            jax.ShapeDtypeStruct((3, 2 * FC), F32),
        ],
        scratch_shapes=[pltpu.VMEM((HALF, D), BF16)]
        + [pltpu.VMEM(part.shape, BF16) for part in sums]
        + [
            pltpu.VMEM((512, FC), F32),
            pltpu.VMEM((512, FC), F32),
            pltpu.SemaphoreType.DMA((COUNT + 1,)),
            pltpu.SemaphoreType.DMA((COUNT + 1,)),
        ],
        compiler_params=pltpu.CompilerParams(vmem_limit_bytes=60 * 2**20),
    )(gin, taps, *sums)


def per_device(inputs, pre_gate, pre_up, cotangent, w_gate, w_up, taps_gate, taps_up):
    count = LEN * lax.axis_size("rep") * lax.axis_size("fs")
    factor = float(count) ** (-0.5)
    grad_inputs, taps, *sums = fused(
        inputs[0], pre_gate[0], pre_up[0], cotangent[0],
        w_gate.reshape(4, 2, 64, FC), w_up.reshape(4, 2, 64, FC), taps_gate, taps_up,
    )
    grad_inputs, grad_gate, grad_up, grad_taps_gate, grad_taps_up = finished(factor, grad_inputs, taps, sums)
    return grad_inputs[None], grad_gate, grad_up, grad_taps_gate, grad_taps_up


def solution(mesh):
    placed = (
        P(("rep", "fs"), "tp", None),
        P(("rep", "fs"), None, "tp"),
        P(("rep", "fs"), None, "tp"),
        P(("rep", "fs"), None, "tp"),
        P("fs", "tp"),
        P("fs", "tp"),
        P(),
        P(),
    )
    return jax.shard_map(
        per_device,
        mesh=mesh,
        in_specs=placed,
        out_specs=(P(("rep", "fs"), "tp", None), P("fs", "tp"), P("fs", "tp"), P(), P()),
        check_vma=False,
    )
```

```python
import functools

import jax
import jax.numpy as jnp
from jax import lax
from jax.experimental import pallas as pl
from jax.experimental.pallas import tpu as pltpu
from jax.sharding import PartitionSpec as P

F32 = jnp.float32
BF16 = jnp.bfloat16
MESH = pl.DeviceIdType.MESH

Y1, Y3, X1, X3, Z1, Z3 = range(6)
CYCLE = (X1, Z1, X3, Z3, Y1, Y3)
REP_CYCLE = (X1, Z1, X3, Z3)
GROUPS = ((0, 512), (512, 512), (1024, 384))
SPLIT = 2
SUB = 32
ROWS = SUB // SPLIT
PORTIONS = tuple((group, mat, h) for group in range(len(GROUPS)) for mat in range(2) for h in range(SPLIT))
COUNT = len(PORTIONS)
GROUP_ORDER = (0, 1, 2)
ORDERS = (
    (Z1, X1, X3, Y1, Z3, Y3), (Z3, X1, Y1, Y3, Z1, X3), (X1, Y3, Z3, Z1, X3, Y1), (X3, Z3, Z1, Y1, X1, Y3),
    (Y1, X1, Z1, Z3, Y3, X3), (X3, Z3, X1, Y1, Y3, Z1), (Z3, X3, Z1, Y3, Y1, X1), (X1, Y3, X3, Z1, Z3, Y1),
    (Z3, Z1, X1, Y3, X3, Y1), (Z1, X3, X1, Z3, Y3, Y1), (Y1, Z1, X3, X1, Y3, Z3), (Y3, Z1, X3, Z3, X1, Y1),
)
AG_ORDERS = (
    (X3, Z1, X1, Z3), (Z1, Z3, X3, X1), (X3, X1, Z3, Z1), (Z1, Z3, X3, X1), (Z3, X1, Z1, X3),
    (Z3, X3, X1, Z1), (Z3, X3, Z1, X1), (Z1, Z3, X1, X3), (X1, X3, Z1, Z3), (X1, Z1, Z3, X3),
    (Z1, X1, X3, Z3), (Z3, X3, X1, Z1),
)
DIRECT = ((0, 0), (1, 3))
LEN = 768
HALF = 384
D = 2048
FC = 1408
STEP = 1024
W_PATHS = ((Y1, Y3), (Y3, Y1))
MASK = {Y1: 1, Y3: 3}


def recv_offset(stage):
    return 64 - 2 ** (6 - stage)


START, ELEM, TURN, PROD, RS, AG, WY, WF, TAP, BACK, FIN = range(11)
NAMES = ("start", "elem", "turn", "prod", "rs", "ag", "wy", "wf", "tap", "back", "fin")
SCHEDULE = (
    (ELEM, 0, 0, 1), (TURN, 0), (START,), (WY, 0, 0, Y1, 2, 0), (WY, 1, 0, Y3, 1, 0), (ELEM, 0, 1, 4),
    (WY, 0, 0, Y1, 0, 0), (WY, 0, 0, Y3, 2, 0), (TURN, 1), (PROD, 0, 0), (WY, 0, 0, Y1, 3, 0),
    (WY, 1, 0, Y3, 3, 0), (WF, 1, 3, 1), (PROD, 0, 1), (ELEM, 1, 0, 2), (WY, 1, 0, Y1, 0, 0),
    (WY, 1, 0, Y3, 0, 0), (ELEM, 1, 2, 4), (PROD, 1, 0), (WY, 0, 0, Y3, 1, 0), (PROD, 1, 1), (ELEM, 2, 0, 1),
    (WF, 0, 1, 2), (ELEM, 2, 1, 3), (WY, 0, 0, Y3, 0, 0), (PROD, 2, 0), (TAP, -1), (PROD, 2, 1), (RS, 0, 0),
    (RS, 2, 0), (RS, 1, 0), (BACK, 0, 0), (RS, 3, 0), (BACK, 0, 1), (FIN, 0, 0), (FIN, 0, 1), (RS, 4, 0),
    (WF, 0, 3, 2), (RS, 6, 0), (RS, 9, 0), (TAP, 0), (RS, 7, 0), (RS, 11, 0), (WY, 1, 0, Y1, 1, 0),
    (RS, 5, 0), (RS, 10, 0), (WY, 0, 0, Y1, 1, 0), (RS, 0, 1), (RS, 2, 1), (RS, 8, 0), (RS, 11, 1),
    (RS, 6, 1), (WY, 1, 0, Y1, 2, 0), (WY, 1, 0, Y3, 2, 0), (TAP, 1), (RS, 1, 1), (RS, 10, 1), (RS, 9, 1),
    (RS, 3, 1), (RS, 7, 1), (WY, 0, 1, Y3, 1, 0), (RS, 0, 2), (RS, 8, 1), (RS, 11, 2), (RS, 4, 1),
    (WY, 1, 0, Y1, 3, 0), (WY, 0, 1, Y3, 2, 0), (RS, 5, 1), (WF, 0, 1, 3), (WF, 0, 1, 1), (RS, 6, 2),
    (RS, 10, 2), (RS, 1, 2), (RS, 9, 2), (RS, 0, 3), (RS, 2, 2), (TAP, 2), (WY, 1, 3, Y1, 0, 0), (RS, 3, 2),
    (RS, 11, 3), (RS, 7, 2), (RS, 8, 2), (WF, 0, 3, 1), (WF, 1, 3, 0), (WF, 1, 3, 2), (RS, 4, 2), (RS, 5, 2),
    (WY, 0, 0, Y3, 3, 0), (RS, 2, 3), (RS, 6, 3), (RS, 10, 3), (RS, 11, 4), (RS, 9, 3), (RS, 7, 3),
    (WF, 1, 1, 0), (RS, 0, 4), (RS, 1, 3), (WF, 0, 2, 1), (RS, 8, 3), (WF, 1, 1, 2), (RS, 4, 3),
    (WY, 1, 3, Y1, 1, 0), (TAP, 3), (RS, 3, 3), (RS, 7, 4), (RS, 5, 3), (RS, 2, 4), (RS, 1, 4), (RS, 6, 4),
    (WY, 0, 1, Y3, 0, 0), (RS, 11, 5), (WF, 1, 2, 0), (WF, 0, 3, 3), (WF, 1, 1, 1), (RS, 10, 4),
    (WF, 0, 2, 2), (RS, 9, 4), (RS, 0, 5), (WY, 1, 3, Y1, 2, 0), (RS, 4, 4), (AG, 11, 0), (RS, 3, 4),
    (RS, 5, 4), (RS, 6, 5), (RS, 8, 4), (RS, 1, 5), (WY, 0, 1, Y3, 3, 0), (RS, 7, 5), (RS, 2, 5), (RS, 9, 5),
    (WY, 1, 3, Y1, 3, 0), (WF, 1, 2, 1), (RS, 10, 5), (AG, 6, 0), (RS, 3, 5), (TAP, 4), (AG, 9, 0),
    (WY, 1, 0, Y3, 3, 1), (AG, 0, 0), (RS, 4, 5), (RS, 5, 5), (WF, 1, 2, 2), (AG, 11, 1), (RS, 8, 5),
    (AG, 1, 0), (AG, 2, 0), (AG, 7, 0), (AG, 10, 0), (WY, 0, 0, Y1, 0, 1), (AG, 3, 0), (AG, 9, 1), (AG, 4, 0),
    (AG, 0, 1), (WF, 0, 2, 3), (AG, 5, 0), (WY, 0, 0, Y3, 0, 1), (AG, 1, 1), (AG, 11, 2), (AG, 8, 0),
    (AG, 7, 1), (AG, 2, 1), (AG, 3, 1), (WY, 1, 0, Y1, 3, 1), (TAP, 5), (AG, 10, 1), (AG, 6, 1), (AG, 4, 1),
    (AG, 5, 1), (AG, 9, 2), (BACK, 3, 1), (AG, 0, 2), (AG, 1, 2), (AG, 8, 1), (WY, 0, 1, Y3, 0, 1),
    (BACK, 1, 0), (WY, 1, 3, Y1, 3, 1), (AG, 7, 2), (AG, 3, 2), (FIN, 3, 1), (AG, 11, 3), (AG, 6, 2),
    (AG, 5, 2), (BACK, 3, 0), (AG, 2, 2), (AG, 4, 2), (AG, 10, 2), (FIN, 1, 0), (BACK, 1, 1), (AG, 8, 2),
    (AG, 9, 3), (AG, 1, 3), (FIN, 3, 0), (AG, 0, 3), (BACK, 2, 0), (AG, 7, 3), (AG, 5, 3), (FIN, 1, 1),
    (AG, 3, 3), (BACK, 2, 1), (AG, 10, 3), (FIN, 2, 0), (AG, 4, 3), (AG, 2, 3), (AG, 8, 3), (AG, 6, 3),
    (FIN, 2, 1),
)


def kernel(
    x_hbm, gate_hbm, up_hbm, cot_hbm, wg_hbm, wu_hbm, kg_ref, ku_ref,
    gin_hbm, taps_hbm, *rest,
):
    sums, (xs, xt, act_g, act_u, act_c, ws_g, ws_u, *scratch) = rest[:COUNT], rest[COUNT:]
    gs, rs, ags = (scratch[i * COUNT : (i + 1) * COUNT] for i in range(3))
    (
        tap, tap_in, tap_out, part, part_in,
        load_sem, rs_send, rs_recv, ag_send, ag_recv, w_send, wy_recv, wf_recv,
        t_send, t_recv, x_send, x_recv, o_send, o_recv, out_sem, sum_sem,
    ) = scratch[3 * COUNT :]
    ws = (ws_g, ws_u)
    acts = (act_g, act_u)
    rep, y, tp = lax.axis_index("rep"), lax.axis_index("fs"), lax.axis_index("tp")
    z, x = rep // 4, rep % 4

    def gray(c):
        return (c + c // 2) % 2, c // 2

    bits = gray(y) + gray(x) + gray(z)

    def flip1(c):
        return c + 1 - 2 * (c % 2)

    peers = (
        {"fs": flip1(y)}, {"fs": 3 - y},
        {"rep": z * 4 + flip1(x)}, {"rep": z * 4 + 3 - x},
        {"rep": flip1(z) * 4 + x}, {"rep": (3 - z) * 4 + x},
    )
    other_core = {"tp": 1 - tp}

    def remote(src, dst, send, recv, peer):
        return pltpu.make_async_remote_copy(
            src_ref=src, dst_ref=dst, send_sem=send, recv_sem=recv, device_id=peer, device_id_type=MESH
        )

    def send(copy):
        copy.start()

    loads = {}

    def load(name, src, dst):
        copy = pltpu.make_async_copy(src, dst, load_sem.at[len(loads)])
        copy.start()
        loads[name] = copy

    def load_group(key, first, size):
        for name, src, dst in (("g", gate_hbm, act_g), ("u", up_hbm, act_u), ("c", cot_hbm, act_c)):
            load(name + str(key), src.at[:, pl.ds(first, size)], dst.at[:, pl.ds(first, size)])

    barrier = pltpu.get_barrier_semaphore()
    for peer in peers + (other_core,):
        pl.semaphore_signal(barrier, inc=1, device_id=peer, device_id_type=MESH)
    load_group("first", 0, 128)
    load_group(0, 128, GROUPS[0][1] - 128)
    load("x", x_hbm, xs.at[tp])
    for mat, src in enumerate((wg_hbm, wu_hbm)):
        load("w" + str(mat), src, ws[mat].at[0])
    for group in range(1, len(GROUPS)):
        load_group(group, *GROUPS[group])
    tap[0] = jnp.zeros((8, FC), F32)

    parity = (x % 2, z % 2)

    waited = set()

    def wy_copy(mat, src_mask, dim, link, far):
        dst_mask = src_mask ^ MASK[dim]
        at = (mat * 3 + dst_mask - 1) * 4 + link
        half = parity[link // 2]
        if far:
            at, half = 24 + DIRECT.index((mat, link)) * 3 + dst_mask - 1, 1 - half
        return remote(
            ws[mat].at[src_mask, link, half], ws[mat].at[dst_mask, link, half],
            w_send.at[mat], wy_recv.at[at], peers[dim],
        )

    def wf_copy(mat, mask, link):
        half = ws[mat].at[mask, link, parity[link // 2]]
        at = (mask - 1) * 2 + link // 2
        return remote(half, half, w_send.at[mat], wf_recv.at[at], peers[2 + link])

    def landed(ref, sem):
        pltpu.make_async_copy(ref, ref, sem).wait()

    def wf_wait(mask, n):
        count = 4 - sum(link // 2 == n for _, link in DIRECT)
        if count:
            landed(ws[0].at[pl.ds(0, count), 0, 0], wf_recv.at[(mask - 1) * 2 + n])

    def wy_wait(mat, mask, link, far):
        first, second = W_PATHS[mat]
        dim, src = {MASK[first]: (first, 0), MASK[second]: (second, 0), 2: (second, MASK[first])}[mask]
        if (mat, mask, link, far) not in waited:
            waited.add((mat, mask, link, far))
            wy_copy(mat, src, dim, link, far).wait_recv()

    def own_loaded(mat):
        if mat not in waited:
            waited.add(mat)
            loads["w" + str(mat)].wait()

    def wy_step(mat, src_mask, dim, link, far):
        if src_mask:
            wy_wait(mat, src_mask, link, far)
        else:
            own_loaded(mat)
        send(wy_copy(mat, src_mask, dim, link, far))

    def wf_step(mat, mask, link):
        wy_wait(mat, mask, link, 0)
        send(wf_copy(mat, mask, link))

    row = lax.broadcasted_iota(jnp.int32, (8, 128), 0)

    def past(value, steps):
        turned = pltpu.roll(value, steps, 0)
        return jnp.concatenate([jnp.where(row >= steps, turned[:8], 0.0), turned[8:]], axis=0)

    def ahead(value, steps):
        turned = pltpu.roll(value, LEN - steps, 0)
        return jnp.concatenate([turned[:-8], jnp.where(row < 8 - steps, turned[-8:], 0.0)], axis=0)

    def group_loaded(group):
        if ("group", group) not in waited:
            waited.add(("group", group))
            for name in ("g", "u", "c"):
                loads[name + str(group)].wait()

    def elementwise_block(first, j):
        cols = pl.ds(pl.multiple_of(first + j * 128, 128), 128)
        tap_cols = pl.ds(pl.multiple_of(tp * FC + first + j * 128, 128), 128)
        kg_all = kg_ref[:, tap_cols].astype(F32)
        ku_all = ku_ref[:, tap_cols].astype(F32)
        kg = [kg_all[i : i + 1, :] for i in range(3)]
        ku = [ku_all[i : i + 1, :] for i in range(3)]
        gate = act_g[:, cols].astype(F32)
        gates = (past(gate, 2), past(gate, 1), gate)
        mixed_gate = kg[0] * gates[0] + kg[1] * gates[1] + kg[2] * gates[2]
        up = act_u[:, cols].astype(F32)
        ups = (past(up, 2), past(up, 1), up)
        mixed_up = ku[0] * ups[0] + ku[1] * ups[1] + ku[2] * ups[2]
        scale = (2.0 / 3.141592653589793) ** 0.5
        square = mixed_gate * mixed_gate
        bent = jnp.tanh(mixed_gate * (scale + (scale * 0.044715) * square))
        lift = 0.5 + 0.5 * bent
        slope = lift + mixed_gate * (1.0 - bent * bent) * (0.5 * scale + (1.5 * 0.044715 * scale) * square)
        cot = act_c[:, cols].astype(F32)
        back_up = cot * (mixed_gate * lift)
        back_gate = cot * mixed_up * slope
        dg = kg[2] * back_gate + kg[1] * ahead(back_gate, 1) + kg[0] * ahead(back_gate, 2)
        du = ku[2] * back_up + ku[1] * ahead(back_up, 1) + ku[0] * ahead(back_up, 2)
        act_g[:, cols] = dg.astype(BF16)
        act_u[:, cols] = du.astype(BF16)
        for i in range(3):
            tap[0, pl.ds(i, 1), cols] = jnp.sum(back_gate * gates[i], axis=0, keepdims=True)
            tap[0, pl.ds(3 + i, 1), cols] = jnp.sum(back_up * ups[i], axis=0, keepdims=True)

    def elementwise(group, begin, end):
        if group == 0 and begin == 0:
            group_loaded("first")
            elementwise_block(0, 0)
            begin = 1
        group_loaded(group)

        def block(j, _):
            elementwise_block(GROUPS[group][0], j)
            return 0

        lax.fori_loop(begin, end, block, 0)

    def product_block(group, mat, step):
        first, size = GROUPS[group]
        value = jnp.dot(
            xt[pl.ds(pl.multiple_of(step * STEP, STEP), STEP), :],
            acts[mat][:, pl.ds(first, size)],
            preferred_element_type=F32,
        ).astype(BF16)
        for k in range(STEP // 512):
            low, high = gray(step * (STEP // 512) + k)
            for p in range(COUNT):
                if PORTIONS[p][:2] != (group, mat):
                    continue
                place = {ORDERS[p][s]: 2 ** (5 - s) for s in range(6)}
                base = low * place[Y1] + high * place[Y3]
                for sub in range(16):
                    at = sum(((sub >> i) & 1) * place[2 + i] for i in range(4))
                    row_at = k * 512 + sub * SUB + PORTIONS[p][2] * ROWS
                    gs[p][base + at] = value[row_at : row_at + ROWS, :]

    def product_done(group, mat):
        for p in range(COUNT):
            if PORTIONS[p][:2] == (group, mat):
                send(rs_copy(p, 0))

    def product(group, mat):
        def block(step, _):
            product_block(group, mat, step)
            return 0

        lax.fori_loop(0, D // STEP, block, 0)
        product_done(group, mat)

    def base_of(p, stage):
        return sum(bits[ORDERS[p][s]] * 2 ** (5 - s) for s in range(stage))

    def rs_copy(p, stage):
        dim, count = ORDERS[p][stage], 2 ** (5 - stage)
        start = base_of(p, stage) + (1 - bits[dim]) * count
        at = p * 6 + stage
        return remote(
            gs[p].at[pl.ds(start, count)], rs[p].at[pl.ds(recv_offset(stage), count)],
            rs_send.at[p], rs_recv.at[at], peers[dim],
        )

    def ag_at(p):
        return sum(bits[dim] * 2**t for t, dim in enumerate(AG_ORDERS[p]))

    def ag_copy(p, step):
        count = 2**step
        held = ags[p].at[pl.ds((ag_at(p) // count) * count, count)]
        at = p * 4 + step
        return remote(held, held, ag_send.at[p], ag_recv.at[at], peers[AG_ORDERS[p][step]])

    def rs_step(p, stage):
        rs_copy(p, stage).wait_recv()
        start, count, offset = base_of(p, stage + 1), 2 ** (5 - stage), recv_offset(stage)

        def total(i):
            return (gs[p][start + i].astype(F32) + rs[p][offset + i].astype(F32)).astype(BF16)

        if stage == 5:
            ags[p][ag_at(p)] = total(0)
            send(ag_copy(p, 0))
            return

        def add(i, _):
            gs[p][start + i] = total(i)
            return 0

        lax.fori_loop(0, count, add, 0)
        send(rs_copy(p, stage + 1))

    def ag_step(p, step):
        ag_copy(p, step).wait_recv()
        if step < 3:
            send(ag_copy(p, step + 1))
            return
        pltpu.make_async_copy(ags[p], sums[p], sum_sem.at[PORTIONS[p][0]]).start()

    def tap_copy(step):
        peer = peers[step] if step < 6 else other_core
        return remote(tap.at[step], tap_in.at[step], t_send.at[0], t_recv.at[step], peer)

    def tap_step(step):
        if step >= 0:
            tap_copy(step).wait_recv()
            tap[step + 1] = tap[step] + tap_in[step]
        send(tap_copy(step + 1))

    def back(mask, n):
        for mat in range(2):
            own_loaded(mat)
            for link in (2 * n, 2 * n + 1) if mask else ():
                wy_wait(mat, mask, link, 0)
                if (mat, link) in DIRECT:
                    wy_wait(mat, mask, link, 1)
        if mask:
            wf_wait(mask, n)

        def block(k, _):
            def dot(mat):
                weights = ws[mat][mask, pl.ds(2 * k, 2)].reshape(256, FC)
                return lax.dot_general(
                    acts[mat][...], weights, (((1,), (1,)), ((), ())), preferred_element_type=F32
                )

            value = (dot(0) + dot(1)).astype(BF16)
            part[mask, k, 0] = value[:HALF]
            part[mask, k, 1] = value[HALF:]
            return 0

        lax.fori_loop(n, n + 1 + (tp // 2), block, 0)
        send(part_copy(mask, n))

    def part_copy(mask, n):
        return remote(
            part.at[mask, n, 1 - tp], part_in.at[mask, n], o_send.at[0], o_recv.at[mask * 2 + n], other_core
        )

    def finish(mask, n):
        part_copy(mask, n).wait_recv()
        part_in[mask, n] = (part[mask, n, tp].astype(F32) + part_in[mask, n].astype(F32)).astype(BF16)
        block = {0: y, 1: flip1(y), 2: (y + 2) % 4, 3: 3 - y}[mask]
        cols = pl.ds(pl.multiple_of(block * 512 + n * 256, 256), 256)
        pltpu.make_async_copy(part_in.at[mask, n], gin_hbm.at[:, cols], out_sem.at[0]).start()

    def x_loaded():
        if "x" not in waited:
            waited.add("x")
            loads["x"].wait()

    def turn(second):
        if second:
            x_copy.wait_recv()
        else:
            x_loaded()
        which = 1 - tp if second else tp
        rows = pl.ds(pl.multiple_of(which * HALF, HALF), HALF)

        def block(c, _):
            cols = pl.ds(pl.multiple_of(c * 128, 128), 128)
            xt[cols, rows] = xs[which, :, cols].T
            return 0

        lax.fori_loop(0, D // 128, block, 0)

    def start():
        pl.semaphore_wait(barrier, 7)
        x_loaded()
        send(x_copy)

    x_copy = remote(xs.at[tp], xs.at[tp], x_send.at[0], x_recv.at[0], other_core)
    run = {
        START: start, ELEM: elementwise, TURN: turn, PROD: product, RS: rs_step, AG: ag_step,
        WY: wy_step, WF: wf_step, TAP: tap_step, BACK: back, FIN: finish,
    }
    for op, *numbers in SCHEDULE:
        with jax.named_scope("_".join(str(n) for n in [NAMES[op]] + numbers)):
            run[op](*numbers)
    with jax.named_scope("tail_taps"):
        tap_copy(6).wait_recv()
        tap_out[tp] = tap[6]
        tap_out[1 - tp] = tap_in[6]
        tap_store = pltpu.make_async_copy(tap_out, taps_hbm, out_sem.at[1])
        tap_store.start()
    with jax.named_scope("tail_sends"):
        for p in range(COUNT):
            landed(rs[p], rs_send.at[p])
            landed(ags[p].at[pl.ds(0, 15)], ag_send.at[p])
        for mat in range(2):
            landed(ws[mat].at[pl.ds(0, 3)], w_send.at[mat])
        landed(tap, t_send.at[0])
        landed(part_in, o_send.at[0])
        x_copy.wait_send()
    with jax.named_scope("tail_stores"):
        for group in range(len(GROUPS)):
            landed(gs[group * 2 * SPLIT].at[pl.ds(0, 32 * SPLIT)], sum_sem.at[group])
        landed(part_in, out_sem.at[0])
        tap_store.wait()


def fused(x, gate, up, cot, wg, wu, kg, ku):
    sizes = [GROUPS[group][1] for group, _, _ in PORTIONS]
    any_space = pl.BlockSpec(memory_space=pl.ANY)
    in_vmem = pl.BlockSpec(memory_space=pltpu.VMEM)
    dma = pltpu.SemaphoreType.DMA
    return pl.pallas_call(
        kernel,
        in_specs=[any_space] * 6 + [in_vmem] * 2,
        out_specs=[any_space] * (2 + COUNT),
        out_shape=[jax.ShapeDtypeStruct((HALF, D), BF16), jax.ShapeDtypeStruct((2, 8, FC), F32)]
        + [jax.ShapeDtypeStruct((16, ROWS, size), BF16) for size in sizes],
        scratch_shapes=[
            pltpu.VMEM((2, HALF, D), BF16),
            pltpu.VMEM((D, LEN), BF16),
            pltpu.VMEM((LEN, FC), BF16),
            pltpu.VMEM((LEN, FC), BF16),
            pltpu.VMEM((LEN, FC), BF16),
            pltpu.VMEM((4, 4, 2, 64, FC), BF16),
            pltpu.VMEM((4, 4, 2, 64, FC), BF16),
        ]
        + [pltpu.VMEM((64, ROWS, size), BF16) for size in sizes]
        + [pltpu.VMEM((63, ROWS, size), BF16) for size in sizes]
        + [pltpu.VMEM((16, ROWS, size), BF16) for size in sizes]
        + [
            pltpu.VMEM((7, 8, FC), F32),
            pltpu.VMEM((7, 8, FC), F32),
            pltpu.VMEM((2, 8, FC), F32),
            pltpu.VMEM((4, 2, 2, HALF, 256), BF16),
            pltpu.VMEM((4, 2, HALF, 256), BF16),
            dma((6 + 3 * len(GROUPS),)),
            dma((COUNT,)), dma((6 * COUNT,)), dma((COUNT,)), dma((4 * COUNT,)),
            dma((2,)), dma((24 + 3 * len(DIRECT),)), dma((6,)),
            dma((1,)), dma((7,)), dma((1,)), dma((1,)), dma((1,)), dma((8,)), dma((2,)), dma((len(GROUPS),)),
        ],
        compiler_params=pltpu.CompilerParams(
            collective_id=0, has_side_effects=True, vmem_limit_bytes=67043328
        ),
        cost_estimate=pl.CostEstimate(flops=18 * 10**9, bytes_accessed=20 * 2**20, transcendentals=10**6),
    )(x, gate, up, cot, wg, wu, kg, ku)


def finish_kernel(factor, gin_hbm, taps_ref, *rest):
    sums, rest = rest[:COUNT], rest[COUNT:]
    gin_out, gate_out, up_out, tap_gate, tap_up, gin, *rest = rest
    held, (wide_gate, wide_up, in_sem, out_sem) = rest[:COUNT], rest[COUNT:]
    wide, results = (wide_gate, wide_up), (gate_out, up_out)
    gin_in = pltpu.make_async_copy(gin_hbm, gin, in_sem.at[COUNT])
    gin_in.start()
    copies = [pltpu.make_async_copy(sums[p], held[p], in_sem.at[p]) for p in range(COUNT)]
    for copy in copies:
        copy.start()
    for i in range(2):
        cols = pl.ds(i * FC, FC)
        tap_gate[:, cols] = factor * taps_ref[i, :3, :]
        tap_up[:, cols] = factor * taps_ref[i, 3:6, :]
    gin_in.wait()
    outs = [pltpu.make_async_copy(gin, gin_out, out_sem.at[0])]
    outs[0].start()
    for p in range(COUNT):
        with jax.named_scope("sum_wait_" + str(p)):
            copies[p].wait()
        group, mat, h = PORTIONS[p]
        first, size = GROUPS[group]
        for sub in range(16):
            at = sum(((sub >> (dim - 2)) & 1) * 2**t for t, dim in enumerate(AG_ORDERS[p]))
            rows = pl.ds(sub * SUB + h * ROWS, ROWS)
            wide[mat][rows, pl.ds(first, size)] = factor * held[p][at].astype(F32)
        if h == SPLIT - 1:
            cols = pl.ds(first, size)
            copy = pltpu.make_async_copy(wide[mat].at[:, cols], results[mat].at[:, cols], out_sem.at[len(outs)])
            copy.start()
            outs.append(copy)
    with jax.named_scope("last_wait"):
        for copy in outs:
            copy.wait()


def finished(factor, gin, taps, sums):
    any_space = pl.BlockSpec(memory_space=pl.ANY)
    in_vmem = pl.BlockSpec(memory_space=pltpu.VMEM)
    return pl.pallas_call(
        functools.partial(finish_kernel, factor),
        in_specs=[any_space, in_vmem] + [any_space] * COUNT,
        out_specs=[any_space] * 3 + [in_vmem] * 2,
        out_shape=[
            jax.ShapeDtypeStruct((HALF, D), BF16),
            jax.ShapeDtypeStruct((512, FC), F32),
            jax.ShapeDtypeStruct((512, FC), F32),
            jax.ShapeDtypeStruct((3, 2 * FC), F32),
            jax.ShapeDtypeStruct((3, 2 * FC), F32),
        ],
        scratch_shapes=[pltpu.VMEM((HALF, D), BF16)]
        + [pltpu.VMEM(part.shape, BF16) for part in sums]
        + [
            pltpu.VMEM((512, FC), F32),
            pltpu.VMEM((512, FC), F32),
            pltpu.SemaphoreType.DMA((COUNT + 1,)),
            pltpu.SemaphoreType.DMA((COUNT + 1,)),
        ],
        compiler_params=pltpu.CompilerParams(vmem_limit_bytes=60 * 2**20),
    )(gin, taps, *sums)


def per_device(inputs, pre_gate, pre_up, cotangent, w_gate, w_up, taps_gate, taps_up):
    count = LEN * lax.axis_size("rep") * lax.axis_size("fs")
    factor = float(count) ** (-0.5)
    grad_inputs, taps, *sums = fused(
        inputs[0], pre_gate[0], pre_up[0], cotangent[0],
        w_gate.reshape(4, 2, 64, FC), w_up.reshape(4, 2, 64, FC), taps_gate, taps_up,
    )
    grad_inputs, grad_gate, grad_up, grad_taps_gate, grad_taps_up = finished(factor, grad_inputs, taps, sums)
    return grad_inputs[None], grad_gate, grad_up, grad_taps_gate, grad_taps_up


def solution(mesh):
    placed = (
        P(("rep", "fs"), "tp", None),
        P(("rep", "fs"), None, "tp"),
        P(("rep", "fs"), None, "tp"),
        P(("rep", "fs"), None, "tp"),
        P("fs", "tp"),
        P("fs", "tp"),
        P(),
        P(),
    )
    return jax.shard_map(
        per_device,
        mesh=mesh,
        in_specs=placed,
        out_specs=(P(("rep", "fs"), "tp", None), P("fs", "tp"), P("fs", "tp"), P(), P()),
        check_vma=False,
    )
```

```python
import functools

import jax
import jax.numpy as jnp
from jax import lax
from jax.experimental import pallas as pl
from jax.experimental.pallas import tpu as pltpu
from jax.sharding import PartitionSpec as P

F32 = jnp.float32
BF16 = jnp.bfloat16
MESH = pl.DeviceIdType.MESH

Y1, Y3, X1, X3, Z1, Z3 = range(6)
CYCLE = (X1, Z1, X3, Z3, Y1, Y3)
REP_CYCLE = (X1, Z1, X3, Z3)
GROUPS = ((0, 512), (512, 512), (1024, 384))
SPLIT = 2
SUB = 32
ROWS = SUB // SPLIT
PORTIONS = tuple((group, mat, h) for group in range(len(GROUPS)) for mat in range(2) for h in range(SPLIT))
COUNT = len(PORTIONS)
GROUP_ORDER = (0, 1, 2)
ORDERS = (
    (Z3, X3, Y3, X1, Z1, Y1), (Z1, X3, X1, Y3, Z3, Y1), (X1, Y3, Z3, X3, Y1, Z1), (X3, X1, Z1, Z3, Y1, Y3),
    (Y3, Z1, X3, Z3, X1, Y1), (Z1, X3, Z3, X1, Y3, Y1), (X3, Z3, Z1, X1, Y3, Y1), (Z3, Y1, X3, X1, Y3, Z1),
    (X1, Z1, X3, Y3, Y1, Z3), (Y1, Z3, X1, Y3, X3, Z1), (Y1, Z1, Z3, X1, X3, Y3), (Z3, X1, Y1, Y3, X3, Z1),
)
AG_ORDERS = (
    (X1, Z1, Z3, X3), (X3, Z1, Z3, X1), (X1, X3, Z3, Z1), (X3, Z1, X1, Z3), (Z3, X1, X3, Z1),
    (X3, Z3, Z1, X1), (X1, X3, Z1, Z3), (Z1, Z3, X3, X1), (Z1, X1, Z3, X3), (Z3, X1, Z1, X3),
    (Z3, X1, Z1, X3), (Z1, X3, X1, Z3),
)
DIRECT = ((0, 1), (1, 3))
LEN = 768
HALF = 384
D = 2048
FC = 1408
STEP = 1024
W_PATHS = ((Y1, Y3), (Y3, Y1))
MASK = {Y1: 1, Y3: 3}


def recv_offset(stage):
    return 64 - 2 ** (6 - stage)


START, ELEM, TURN, PROD, RS, AG, WY, WF, TAP, BACK, FIN = range(11)
NAMES = ("start", "elem", "turn", "prod", "rs", "ag", "wy", "wf", "tap", "back", "fin")
SCHEDULE = (
    (ELEM, 0, 0, 2), (START,), (WY, 0, 0, Y1, 1, 0), (WY, 1, 0, Y3, 1, 0), (ELEM, 0, 2, 4), (TURN, 0),
    (WY, 0, 0, Y1, 2, 0), (WY, 0, 0, Y3, 0, 0), (TURN, 1), (PROD, 0, 0), (WY, 0, 0, Y1, 3, 0),
    (WY, 1, 0, Y3, 0, 0), (PROD, 0, 1), (ELEM, 1, 0, 2), (WY, 1, 0, Y1, 0, 0), (WY, 0, 1, Y3, 1, 0),
    (ELEM, 1, 2, 4), (PROD, 1, 0), (WY, 1, 3, Y1, 1, 0), (PROD, 1, 1), (ELEM, 2, 0, 1), (ELEM, 2, 1, 3),
    (WY, 1, 3, Y1, 0, 0), (WF, 1, 3, 0), (PROD, 2, 0), (TAP, -1), (PROD, 2, 1), (BACK, 0, 0), (BACK, 0, 1),
    (RS, 1, 0), (RS, 0, 0), (WY, 0, 0, Y3, 1, 0), (FIN, 0, 0), (RS, 2, 0), (RS, 3, 0), (FIN, 0, 1),
    (WF, 0, 1, 2), (RS, 4, 0), (RS, 5, 0), (RS, 7, 0), (RS, 6, 0), (RS, 9, 0), (RS, 8, 0),
    (WY, 0, 0, Y3, 2, 0), (TAP, 0), (WF, 1, 2, 0), (RS, 2, 1), (RS, 1, 1), (WY, 0, 1, Y3, 2, 0), (RS, 11, 0),
    (RS, 3, 1), (RS, 4, 1), (RS, 10, 0), (WY, 0, 1, Y3, 3, 0), (TAP, 1), (RS, 0, 1), (RS, 8, 1), (RS, 6, 1),
    (WY, 1, 0, Y1, 2, 0), (RS, 1, 2), (RS, 3, 2), (WF, 1, 1, 0), (RS, 7, 1), (WY, 1, 0, Y1, 1, 0), (RS, 9, 1),
    (RS, 5, 1), (RS, 11, 1), (WY, 0, 0, Y3, 3, 0), (WF, 0, 2, 2), (RS, 10, 1), (RS, 2, 2), (TAP, 2),
    (RS, 4, 2), (RS, 0, 2), (RS, 3, 3), (RS, 1, 3), (RS, 6, 2), (RS, 8, 2), (WF, 0, 3, 2),
    (WY, 0, 0, Y1, 0, 0), (WY, 1, 0, Y3, 2, 0), (RS, 5, 2), (WF, 1, 3, 1), (WF, 0, 1, 3), (RS, 9, 2),
    (RS, 7, 2), (RS, 11, 2), (RS, 10, 2), (RS, 0, 3), (RS, 2, 3), (RS, 3, 4), (RS, 8, 3), (RS, 4, 3),
    (WF, 1, 1, 2), (RS, 6, 3), (RS, 1, 4), (WF, 1, 1, 1), (TAP, 3), (WF, 0, 3, 3), (WY, 1, 0, Y1, 3, 1),
    (RS, 5, 3), (WF, 0, 3, 0), (RS, 0, 4), (RS, 7, 3), (RS, 2, 4), (RS, 8, 4), (RS, 10, 3), (RS, 9, 3),
    (RS, 1, 5), (WY, 1, 0, Y3, 3, 0), (RS, 4, 4), (WF, 1, 3, 2), (WF, 0, 2, 3), (RS, 11, 3), (WF, 0, 1, 0),
    (RS, 3, 5), (WY, 1, 3, Y1, 2, 0), (RS, 6, 4), (WF, 1, 2, 1), (RS, 5, 4), (RS, 7, 4), (RS, 2, 5),
    (RS, 10, 4), (RS, 8, 5), (RS, 0, 5), (RS, 9, 4), (WY, 0, 1, Y3, 0, 0), (TAP, 4), (RS, 4, 5), (AG, 1, 0),
    (RS, 11, 4), (AG, 3, 0), (WY, 0, 0, Y1, 1, 1), (RS, 10, 5), (RS, 7, 5), (AG, 8, 0), (WY, 1, 0, Y3, 3, 1),
    (RS, 9, 5), (AG, 2, 0), (RS, 6, 5), (AG, 0, 0), (AG, 1, 1), (RS, 5, 5), (AG, 4, 0), (RS, 11, 5), (TAP, 5),
    (WY, 1, 3, Y1, 3, 0), (AG, 10, 0), (AG, 3, 1), (WF, 1, 2, 2), (AG, 7, 0), (AG, 8, 1), (AG, 9, 0),
    (AG, 6, 0), (AG, 2, 1), (AG, 5, 0), (AG, 0, 1), (WY, 0, 0, Y3, 1, 1), (AG, 11, 0), (AG, 4, 1), (AG, 1, 2),
    (AG, 10, 1), (BACK, 1, 0), (WY, 1, 0, Y1, 3, 0), (AG, 6, 1), (AG, 7, 1), (AG, 8, 2), (AG, 3, 2),
    (WF, 0, 2, 0), (AG, 9, 1), (AG, 11, 1), (BACK, 3, 1), (WY, 0, 1, Y3, 1, 1), (FIN, 1, 0), (AG, 5, 1),
    (AG, 4, 2), (AG, 2, 2), (AG, 10, 2), (WY, 1, 3, Y1, 3, 1), (AG, 1, 3), (FIN, 3, 1), (AG, 0, 2),
    (AG, 7, 2), (AG, 6, 2), (BACK, 3, 0), (AG, 9, 2), (AG, 8, 3), (BACK, 1, 1), (FIN, 3, 0), (AG, 5, 2),
    (AG, 3, 3), (AG, 10, 3), (AG, 11, 2), (BACK, 2, 0), (FIN, 1, 1), (AG, 6, 3), (AG, 4, 3), (BACK, 2, 1),
    (FIN, 2, 0), (AG, 0, 3), (AG, 7, 3), (AG, 2, 3), (AG, 11, 3), (AG, 9, 3), (FIN, 2, 1), (AG, 5, 3),
)


def kernel(
    x_hbm, gate_hbm, up_hbm, cot_hbm, wg_hbm, wu_hbm, kg_ref, ku_ref,
    gin_hbm, taps_hbm, *rest,
):
    sums, (xs, xt, act_g, act_u, act_c, ws_g, ws_u, *scratch) = rest[:COUNT], rest[COUNT:]
    gs, rs, ags = (scratch[i * COUNT : (i + 1) * COUNT] for i in range(3))
    (
        tap, tap_in, tap_out, part, part_in,
        load_sem, rs_send, rs_recv, ag_send, ag_recv, w_send, wy_recv, wf_recv,
        t_send, t_recv, x_send, x_recv, o_send, o_recv, out_sem, sum_sem,
    ) = scratch[3 * COUNT :]
    ws = (ws_g, ws_u)
    acts = (act_g, act_u)
    rep, y, tp = lax.axis_index("rep"), lax.axis_index("fs"), lax.axis_index("tp")
    z, x = rep // 4, rep % 4

    def gray(c):
        return (c + c // 2) % 2, c // 2

    bits = gray(y) + gray(x) + gray(z)

    def flip1(c):
        return c + 1 - 2 * (c % 2)

    peers = (
        {"fs": flip1(y)}, {"fs": 3 - y},
        {"rep": z * 4 + flip1(x)}, {"rep": z * 4 + 3 - x},
        {"rep": flip1(z) * 4 + x}, {"rep": (3 - z) * 4 + x},
    )
    other_core = {"tp": 1 - tp}

    def remote(src, dst, send, recv, peer):
        return pltpu.make_async_remote_copy(
            src_ref=src, dst_ref=dst, send_sem=send, recv_sem=recv, device_id=peer, device_id_type=MESH
        )

    def send(copy):
        copy.start()

    loads = {}

    def load(name, src, dst):
        copy = pltpu.make_async_copy(src, dst, load_sem.at[len(loads)])
        copy.start()
        loads[name] = copy

    def load_group(key, first, size):
        for name, src, dst in (("g", gate_hbm, act_g), ("u", up_hbm, act_u), ("c", cot_hbm, act_c)):
            load(name + str(key), src.at[:, pl.ds(first, size)], dst.at[:, pl.ds(first, size)])

    barrier = pltpu.get_barrier_semaphore()
    for peer in peers + (other_core,):
        pl.semaphore_signal(barrier, inc=1, device_id=peer, device_id_type=MESH)
    load_group("first", 0, 128)
    load_group(0, 128, GROUPS[0][1] - 128)
    load("x", x_hbm, xs.at[tp])
    for mat, src in enumerate((wg_hbm, wu_hbm)):
        load("w" + str(mat), src, ws[mat].at[0])
    for group in range(1, len(GROUPS)):
        load_group(group, *GROUPS[group])
    tap[0] = jnp.zeros((8, FC), F32)

    parity = (x % 2, z % 2)

    waited = set()

    def wy_copy(mat, src_mask, dim, link, far):
        dst_mask = src_mask ^ MASK[dim]
        at = (mat * 3 + dst_mask - 1) * 4 + link
        half = parity[link // 2]
        if far:
            at, half = 24 + DIRECT.index((mat, link)) * 3 + dst_mask - 1, 1 - half
        return remote(
            ws[mat].at[src_mask, link, half], ws[mat].at[dst_mask, link, half],
            w_send.at[mat], wy_recv.at[at], peers[dim],
        )

    def wf_copy(mat, mask, link):
        half = ws[mat].at[mask, link, parity[link // 2]]
        at = (mask - 1) * 2 + link // 2
        return remote(half, half, w_send.at[mat], wf_recv.at[at], peers[2 + link])

    def landed(ref, sem):
        pltpu.make_async_copy(ref, ref, sem).wait()

    def wf_wait(mask, n):
        count = 4 - sum(link // 2 == n for _, link in DIRECT)
        if count:
            landed(ws[0].at[pl.ds(0, count), 0, 0], wf_recv.at[(mask - 1) * 2 + n])

    def wy_wait(mat, mask, link, far):
        first, second = W_PATHS[mat]
        dim, src = {MASK[first]: (first, 0), MASK[second]: (second, 0), 2: (second, MASK[first])}[mask]
        if (mat, mask, link, far) not in waited:
            waited.add((mat, mask, link, far))
            wy_copy(mat, src, dim, link, far).wait_recv()

    def own_loaded(mat):
        if mat not in waited:
            waited.add(mat)
            loads["w" + str(mat)].wait()

    def wy_step(mat, src_mask, dim, link, far):
        if src_mask:
            wy_wait(mat, src_mask, link, far)
        else:
            own_loaded(mat)
        send(wy_copy(mat, src_mask, dim, link, far))

    def wf_step(mat, mask, link):
        wy_wait(mat, mask, link, 0)
        send(wf_copy(mat, mask, link))

    row = lax.broadcasted_iota(jnp.int32, (8, 128), 0)

    def past(value, steps):
        turned = pltpu.roll(value, steps, 0)
        return jnp.concatenate([jnp.where(row >= steps, turned[:8], 0.0), turned[8:]], axis=0)

    def ahead(value, steps):
        turned = pltpu.roll(value, LEN - steps, 0)
        return jnp.concatenate([turned[:-8], jnp.where(row < 8 - steps, turned[-8:], 0.0)], axis=0)

    def group_loaded(group):
        if ("group", group) not in waited:
            waited.add(("group", group))
            for name in ("g", "u", "c"):
                loads[name + str(group)].wait()

    def elementwise_block(first, j):
        cols = pl.ds(pl.multiple_of(first + j * 128, 128), 128)
        tap_cols = pl.ds(pl.multiple_of(tp * FC + first + j * 128, 128), 128)
        kg_all = kg_ref[:, tap_cols].astype(F32)
        ku_all = ku_ref[:, tap_cols].astype(F32)
        kg = [kg_all[i : i + 1, :] for i in range(3)]
        ku = [ku_all[i : i + 1, :] for i in range(3)]
        gate = act_g[:, cols].astype(F32)
        gates = (past(gate, 2), past(gate, 1), gate)
        mixed_gate = kg[0] * gates[0] + kg[1] * gates[1] + kg[2] * gates[2]
        up = act_u[:, cols].astype(F32)
        ups = (past(up, 2), past(up, 1), up)
        mixed_up = ku[0] * ups[0] + ku[1] * ups[1] + ku[2] * ups[2]
        scale = (2.0 / 3.141592653589793) ** 0.5
        square = mixed_gate * mixed_gate
        bent = jnp.tanh(mixed_gate * (scale + (scale * 0.044715) * square))
        lift = 0.5 + 0.5 * bent
        slope = lift + mixed_gate * (1.0 - bent * bent) * (0.5 * scale + (1.5 * 0.044715 * scale) * square)
        cot = act_c[:, cols].astype(F32)
        back_up = cot * (mixed_gate * lift)
        back_gate = cot * mixed_up * slope
        dg = kg[2] * back_gate + kg[1] * ahead(back_gate, 1) + kg[0] * ahead(back_gate, 2)
        du = ku[2] * back_up + ku[1] * ahead(back_up, 1) + ku[0] * ahead(back_up, 2)
        act_g[:, cols] = dg.astype(BF16)
        act_u[:, cols] = du.astype(BF16)
        for i in range(3):
            tap[0, pl.ds(i, 1), cols] = jnp.sum(back_gate * gates[i], axis=0, keepdims=True)
            tap[0, pl.ds(3 + i, 1), cols] = jnp.sum(back_up * ups[i], axis=0, keepdims=True)

    def elementwise(group, begin, end):
        if group == 0 and begin == 0:
            group_loaded("first")
            elementwise_block(0, 0)
            begin = 1
        group_loaded(group)

        def block(j, _):
            elementwise_block(GROUPS[group][0], j)
            return 0

        lax.fori_loop(begin, end, block, 0)

    def product_block(group, mat, step):
        first, size = GROUPS[group]
        value = jnp.dot(
            xt[pl.ds(pl.multiple_of(step * STEP, STEP), STEP), :],
            acts[mat][:, pl.ds(first, size)],
            preferred_element_type=F32,
        ).astype(BF16)
        for k in range(STEP // 512):
            low, high = gray(step * (STEP // 512) + k)
            for p in range(COUNT):
                if PORTIONS[p][:2] != (group, mat):
                    continue
                place = {ORDERS[p][s]: 2 ** (5 - s) for s in range(6)}
                base = low * place[Y1] + high * place[Y3]
                for sub in range(16):
                    at = sum(((sub >> i) & 1) * place[2 + i] for i in range(4))
                    row_at = k * 512 + sub * SUB + PORTIONS[p][2] * ROWS
                    gs[p][base + at] = value[row_at : row_at + ROWS, :]

    def product_done(group, mat):
        for p in range(COUNT):
            if PORTIONS[p][:2] == (group, mat):
                send(rs_copy(p, 0))

    def product(group, mat):
        def block(step, _):
            product_block(group, mat, step)
            return 0

        lax.fori_loop(0, D // STEP, block, 0)
        product_done(group, mat)

    def base_of(p, stage):
        return sum(bits[ORDERS[p][s]] * 2 ** (5 - s) for s in range(stage))

    def rs_copy(p, stage):
        dim, count = ORDERS[p][stage], 2 ** (5 - stage)
        start = base_of(p, stage) + (1 - bits[dim]) * count
        at = p * 6 + stage
        return remote(
            gs[p].at[pl.ds(start, count)], rs[p].at[pl.ds(recv_offset(stage), count)],
            rs_send.at[p], rs_recv.at[at], peers[dim],
        )

    def ag_at(p):
        return sum(bits[dim] * 2**t for t, dim in enumerate(AG_ORDERS[p]))

    def ag_copy(p, step):
        count = 2**step
        held = ags[p].at[pl.ds((ag_at(p) // count) * count, count)]
        at = p * 4 + step
        return remote(held, held, ag_send.at[p], ag_recv.at[at], peers[AG_ORDERS[p][step]])

    def rs_step(p, stage):
        rs_copy(p, stage).wait_recv()
        start, count, offset = base_of(p, stage + 1), 2 ** (5 - stage), recv_offset(stage)

        def total(i):
            return (gs[p][start + i].astype(F32) + rs[p][offset + i].astype(F32)).astype(BF16)

        if stage == 5:
            ags[p][ag_at(p)] = total(0)
            send(ag_copy(p, 0))
            return

        def add(i, _):
            gs[p][start + i] = total(i)
            return 0

        lax.fori_loop(0, count, add, 0)
        send(rs_copy(p, stage + 1))

    def ag_step(p, step):
        ag_copy(p, step).wait_recv()
        if step < 3:
            send(ag_copy(p, step + 1))
            return
        pltpu.make_async_copy(ags[p], sums[p], sum_sem.at[PORTIONS[p][0]]).start()

    def tap_copy(step):
        peer = peers[step] if step < 6 else other_core
        return remote(tap.at[step], tap_in.at[step], t_send.at[0], t_recv.at[step], peer)

    def tap_step(step):
        if step >= 0:
            tap_copy(step).wait_recv()
            tap[step + 1] = tap[step] + tap_in[step]
        send(tap_copy(step + 1))

    def back(mask, n):
        for mat in range(2):
            own_loaded(mat)
            for link in (2 * n, 2 * n + 1) if mask else ():
                wy_wait(mat, mask, link, 0)
                if (mat, link) in DIRECT:
                    wy_wait(mat, mask, link, 1)
        if mask:
            wf_wait(mask, n)

        def block(k, _):
            def dot(mat):
                weights = ws[mat][mask, pl.ds(2 * k, 2)].reshape(256, FC)
                return lax.dot_general(
                    acts[mat][...], weights, (((1,), (1,)), ((), ())), preferred_element_type=F32
                )

            value = (dot(0) + dot(1)).astype(BF16)
            part[mask, k, 0] = value[:HALF]
            part[mask, k, 1] = value[HALF:]
            return 0

        lax.fori_loop(n, n + 1 + (tp // 2), block, 0)
        send(part_copy(mask, n))

    def part_copy(mask, n):
        return remote(
            part.at[mask, n, 1 - tp], part_in.at[mask, n], o_send.at[0], o_recv.at[mask * 2 + n], other_core
        )

    def finish(mask, n):
        part_copy(mask, n).wait_recv()
        part_in[mask, n] = (part[mask, n, tp].astype(F32) + part_in[mask, n].astype(F32)).astype(BF16)
        block = {0: y, 1: flip1(y), 2: (y + 2) % 4, 3: 3 - y}[mask]
        cols = pl.ds(pl.multiple_of(block * 512 + n * 256, 256), 256)
        pltpu.make_async_copy(part_in.at[mask, n], gin_hbm.at[:, cols], out_sem.at[0]).start()

    def x_loaded():
        if "x" not in waited:
            waited.add("x")
            loads["x"].wait()

    def turn(second):
        if second:
            x_copy.wait_recv()
        else:
            x_loaded()
        which = 1 - tp if second else tp
        rows = pl.ds(pl.multiple_of(which * HALF, HALF), HALF)

        def block(c, _):
            cols = pl.ds(pl.multiple_of(c * 128, 128), 128)
            xt[cols, rows] = xs[which, :, cols].T
            return 0

        lax.fori_loop(0, D // 128, block, 0)

    def start():
        pl.semaphore_wait(barrier, 7)
        x_loaded()
        send(x_copy)

    x_copy = remote(xs.at[tp], xs.at[tp], x_send.at[0], x_recv.at[0], other_core)
    run = {
        START: start, ELEM: elementwise, TURN: turn, PROD: product, RS: rs_step, AG: ag_step,
        WY: wy_step, WF: wf_step, TAP: tap_step, BACK: back, FIN: finish,
    }
    for op, *numbers in SCHEDULE:
        with jax.named_scope("_".join(str(n) for n in [NAMES[op]] + numbers)):
            run[op](*numbers)
    with jax.named_scope("tail_taps"):
        tap_copy(6).wait_recv()
        tap_out[tp] = tap[6]
        tap_out[1 - tp] = tap_in[6]
        tap_store = pltpu.make_async_copy(tap_out, taps_hbm, out_sem.at[1])
        tap_store.start()
    with jax.named_scope("tail_sends"):
        for p in range(COUNT):
            landed(rs[p], rs_send.at[p])
            landed(ags[p].at[pl.ds(0, 15)], ag_send.at[p])
        for mat in range(2):
            landed(ws[mat].at[pl.ds(0, 3)], w_send.at[mat])
        landed(tap, t_send.at[0])
        landed(part_in, o_send.at[0])
        x_copy.wait_send()
    with jax.named_scope("tail_stores"):
        for group in range(len(GROUPS)):
            landed(gs[group * 2 * SPLIT].at[pl.ds(0, 32 * SPLIT)], sum_sem.at[group])
        landed(part_in, out_sem.at[0])
        tap_store.wait()


def fused(x, gate, up, cot, wg, wu, kg, ku):
    sizes = [GROUPS[group][1] for group, _, _ in PORTIONS]
    any_space = pl.BlockSpec(memory_space=pl.ANY)
    in_vmem = pl.BlockSpec(memory_space=pltpu.VMEM)
    dma = pltpu.SemaphoreType.DMA
    return pl.pallas_call(
        kernel,
        in_specs=[any_space] * 6 + [in_vmem] * 2,
        out_specs=[any_space] * (2 + COUNT),
        out_shape=[jax.ShapeDtypeStruct((HALF, D), BF16), jax.ShapeDtypeStruct((2, 8, FC), F32)]
        + [jax.ShapeDtypeStruct((16, ROWS, size), BF16) for size in sizes],
        scratch_shapes=[
            pltpu.VMEM((2, HALF, D), BF16),
            pltpu.VMEM((D, LEN), BF16),
            pltpu.VMEM((LEN, FC), BF16),
            pltpu.VMEM((LEN, FC), BF16),
            pltpu.VMEM((LEN, FC), BF16),
            pltpu.VMEM((4, 4, 2, 64, FC), BF16),
            pltpu.VMEM((4, 4, 2, 64, FC), BF16),
        ]
        + [pltpu.VMEM((64, ROWS, size), BF16) for size in sizes]
        + [pltpu.VMEM((63, ROWS, size), BF16) for size in sizes]
        + [pltpu.VMEM((16, ROWS, size), BF16) for size in sizes]
        + [
            pltpu.VMEM((7, 8, FC), F32),
            pltpu.VMEM((7, 8, FC), F32),
            pltpu.VMEM((2, 8, FC), F32),
            pltpu.VMEM((4, 2, 2, HALF, 256), BF16),
            pltpu.VMEM((4, 2, HALF, 256), BF16),
            dma((6 + 3 * len(GROUPS),)),
            dma((COUNT,)), dma((6 * COUNT,)), dma((COUNT,)), dma((4 * COUNT,)),
            dma((2,)), dma((24 + 3 * len(DIRECT),)), dma((6,)),
            dma((1,)), dma((7,)), dma((1,)), dma((1,)), dma((1,)), dma((8,)), dma((2,)), dma((len(GROUPS),)),
        ],
        compiler_params=pltpu.CompilerParams(
            collective_id=0, has_side_effects=True, vmem_limit_bytes=67043328
        ),
        cost_estimate=pl.CostEstimate(flops=18 * 10**9, bytes_accessed=20 * 2**20, transcendentals=10**6),
    )(x, gate, up, cot, wg, wu, kg, ku)


def finish_kernel(factor, gin_hbm, taps_ref, *rest):
    sums, rest = rest[:COUNT], rest[COUNT:]
    gin_out, gate_out, up_out, tap_gate, tap_up, gin, *rest = rest
    held, (wide_gate, wide_up, in_sem, out_sem) = rest[:COUNT], rest[COUNT:]
    wide, results = (wide_gate, wide_up), (gate_out, up_out)
    gin_in = pltpu.make_async_copy(gin_hbm, gin, in_sem.at[COUNT])
    gin_in.start()
    copies = [pltpu.make_async_copy(sums[p], held[p], in_sem.at[p]) for p in range(COUNT)]
    for copy in copies:
        copy.start()
    for i in range(2):
        cols = pl.ds(i * FC, FC)
        tap_gate[:, cols] = factor * taps_ref[i, :3, :]
        tap_up[:, cols] = factor * taps_ref[i, 3:6, :]
    gin_in.wait()
    outs = [pltpu.make_async_copy(gin, gin_out, out_sem.at[0])]
    outs[0].start()
    for p in range(COUNT):
        with jax.named_scope("sum_wait_" + str(p)):
            copies[p].wait()
        group, mat, h = PORTIONS[p]
        first, size = GROUPS[group]
        for sub in range(16):
            at = sum(((sub >> (dim - 2)) & 1) * 2**t for t, dim in enumerate(AG_ORDERS[p]))
            rows = pl.ds(sub * SUB + h * ROWS, ROWS)
            wide[mat][rows, pl.ds(first, size)] = factor * held[p][at].astype(F32)
        if h == SPLIT - 1:
            cols = pl.ds(first, size)
            copy = pltpu.make_async_copy(wide[mat].at[:, cols], results[mat].at[:, cols], out_sem.at[len(outs)])
            copy.start()
            outs.append(copy)
    with jax.named_scope("last_wait"):
        for copy in outs:
            copy.wait()


def finished(factor, gin, taps, sums):
    any_space = pl.BlockSpec(memory_space=pl.ANY)
    in_vmem = pl.BlockSpec(memory_space=pltpu.VMEM)
    return pl.pallas_call(
        functools.partial(finish_kernel, factor),
        in_specs=[any_space, in_vmem] + [any_space] * COUNT,
        out_specs=[any_space] * 3 + [in_vmem] * 2,
        out_shape=[
            jax.ShapeDtypeStruct((HALF, D), BF16),
            jax.ShapeDtypeStruct((512, FC), F32),
            jax.ShapeDtypeStruct((512, FC), F32),
            jax.ShapeDtypeStruct((3, 2 * FC), F32),
            jax.ShapeDtypeStruct((3, 2 * FC), F32),
        ],
        scratch_shapes=[pltpu.VMEM((HALF, D), BF16)]
        + [pltpu.VMEM(part.shape, BF16) for part in sums]
        + [
            pltpu.VMEM((512, FC), F32),
            pltpu.VMEM((512, FC), F32),
            pltpu.SemaphoreType.DMA((COUNT + 1,)),
            pltpu.SemaphoreType.DMA((COUNT + 1,)),
        ],
        compiler_params=pltpu.CompilerParams(vmem_limit_bytes=60 * 2**20),
    )(gin, taps, *sums)


def per_device(inputs, pre_gate, pre_up, cotangent, w_gate, w_up, taps_gate, taps_up):
    count = LEN * lax.axis_size("rep") * lax.axis_size("fs")
    factor = float(count) ** (-0.5)
    grad_inputs, taps, *sums = fused(
        inputs[0], pre_gate[0], pre_up[0], cotangent[0],
        w_gate.reshape(4, 2, 64, FC), w_up.reshape(4, 2, 64, FC), taps_gate, taps_up,
    )
    grad_inputs, grad_gate, grad_up, grad_taps_gate, grad_taps_up = finished(factor, grad_inputs, taps, sums)
    return grad_inputs[None], grad_gate, grad_up, grad_taps_gate, grad_taps_up


def solution(mesh):
    placed = (
        P(("rep", "fs"), "tp", None),
        P(("rep", "fs"), None, "tp"),
        P(("rep", "fs"), None, "tp"),
        P(("rep", "fs"), None, "tp"),
        P("fs", "tp"),
        P("fs", "tp"),
        P(),
        P(),
    )
    return jax.shard_map(
        per_device,
        mesh=mesh,
        in_specs=placed,
        out_specs=(P(("rep", "fs"), "tp", None), P("fs", "tp"), P("fs", "tp"), P(), P()),
        check_vma=False,
    )
```
